32 devices in a mesh: ep: 8 (over z, y), tp: 4 (over x, core).
Axes of the slice: x: 2, y: 2, z: 4, core: 2. Of those that a mesh axis runs over, the one named last changes fastest.
Arguments:
- q_heads: bfloat16 [8192, 1024], P('ep', 'tp'), may hold values from -200 to 200
- k_heads: bfloat16 [8192, 256], P('ep', 'tp'), may hold values from -6 to 6
- v_heads: bfloat16 [8192, 256], P('ep', 'tp'), may hold values from -6 to 6
- sink_logits: float32 [16], P('tp'), may hold values from 1 to 5
- out_weight: bfloat16 [1024, 2048], P(None, 'tp'), may hold values from -1.5 to 1.5
- tokens_b: bfloat16 [4096, 2048], P('ep'), may hold values from -6 to 6
- moe_gain: float32 [2048], replicated, may hold values from 0.1 to 1.9
- router_group: bfloat16 [2048, 4], replicated, may hold values from -0.125 to 0.125
- router_expert: bfloat16 [2048, 16], replicated, may hold values from -0.125 to 0.125
- route_expert: int32 [4096, 2], P('ep'), may hold values from 0 to 15, as said below
- expert_gate: bfloat16 [16, 2048, 1024], P('ep', None, 'tp'), may hold values from -0.125 to 0.125
- expert_up: bfloat16 [16, 2048, 1024], P('ep', None, 'tp'), may hold values from -0.125 to 0.125
- expert_down: bfloat16 [16, 1024, 2048], P('ep', 'tp'), may hold values from -0.75 to 0.75
Outputs:
- mixer_out: bfloat16 [8192, 2048], P('ep', 'tp')
- moe_out: bfloat16 [4096, 2048], P(('ep', 'tp'))
The draws below stay inside these ranges and needn't reach their ends.
Inputs may be any that keep to these rules, and one draw needn't show every extreme that they name: `route_expert`: each token names two different experts, in rising order, of one group of 4 consecutive experts. In each aligned block of 128 rows (the rows of one device) no expert is named by more than 32 tokens, in each group one expert is named by exactly 32 tokens of every block, and each group is named by a quarter of every block's tokens.
All inputs are finite; a program needn't handle non-finite values.
Results may differ from the reference program's by a relative error of at most 0.011.
Values may be sent and summed in bfloat16 or wider, within the bound.
A program may use at most 128 MiB of HBM per device.

```python
import jax
import jax.numpy as jnp
from jax import lax

D = 2048
HEADS = 16
KV = 4
HD = 64
WINDOW = 128
ROW_B = 128
GROUPS = 4
FF = 1024
EXPERTS = 16
GROUP_EXPERTS = 4
CAP = 32
TOK_A = 8192
TOK_B = 4096
N_EP = 8
N_TP = 4


def pair_heads(seed_key):
    key_query, key_keys = jax.random.split(seed_key, 2)
    group_size = HEADS // KV
    queries = jnp.clip(jax.random.normal(key_query, (TOK_A, KV, group_size, HD), jnp.float32), -5.0, 5.0)
    keys_raw = jnp.clip(jax.random.normal(key_keys, (TOK_A, KV, HD), jnp.float32), -5.0, 5.0)
    return (queries.reshape(TOK_A, HEADS * HD), keys_raw.reshape(TOK_A, KV * HD))


def draw_q_heads(key, part):
    return pair_heads(jax.random.fold_in(key, 3))[0].astype(jnp.bfloat16)


def draw_k_heads(key, part):
    return pair_heads(jax.random.fold_in(key, 3))[1].astype(jnp.bfloat16)


def draw_route_expert(key, part):
    block_count = N_EP * N_TP
    half_rows = ROW_B // 2
    quarter_rows = ROW_B // 4
    pool = jnp.repeat(jnp.arange(GROUP_EXPERTS, dtype=jnp.int32), CAP)
    favored = jax.random.randint(jax.random.fold_in(key, 7), (GROUPS,), 0, GROUP_EXPERTS)

    def one_group(group_key, group_index):
        ranks = jax.random.permutation(group_key, pool.shape[0]).astype(jnp.int32)
        ordering = jnp.where(pool == favored[group_index], -1, ranks)
        order = jnp.argsort(ordering, stable=True)
        picked = jnp.sort(pool[order[:half_rows]])
        pairs = jnp.stack([picked[:quarter_rows], picked[quarter_rows:]], axis=1)
        return pairs + group_index * GROUP_EXPERTS

    def one_block(block_key):
        group_keys = jax.random.split(block_key, GROUPS + 1)
        pairs = jax.vmap(one_group)(group_keys[:GROUPS], jnp.arange(GROUPS, dtype=jnp.int32))
        pairs = pairs.reshape(ROW_B, 2)
        return pairs[jax.random.permutation(group_keys[GROUPS], ROW_B)]
    block_keys = jax.random.split(jax.random.fold_in(key, 11), block_count)
    return jax.vmap(one_block)(block_keys).reshape(block_count * ROW_B, 2).astype(jnp.int32)


def block_levels(own_key, dims, cuts, low, largest):
    loudness, own = 1.0, jax.random.fold_in(own_key, 6)
    for axis_at, shards_of in cuts:
        heights = jnp.exp(jax.random.uniform(jax.random.fold_in(own, axis_at), (shards_of,), jnp.float32, low / len(cuts), largest / len(cuts)))
        loudness = loudness * jnp.repeat(heights, dims[axis_at] // shards_of).reshape([-1 if axis == axis_at else 1 for axis in range(len(dims))])
    return loudness


def scatter_about(key, dims, spread, limit, cuts=(), held_as=jnp.bfloat16):
    result = spread * jax.random.normal(key, dims, jnp.float32)
    if cuts:
        result = result * block_levels(key, dims, cuts, -0.22, 0.18)
    return jnp.clip(result, -limit, limit).astype(held_as)


def setup_inputs(seed: int = 0) -> dict:
    key_of = jax.random.split(jax.random.key(seed), 14)
    q_heads = draw_q_heads(jax.random.fold_in(key_of[13], 71), 0)
    k_heads = draw_k_heads(jax.random.fold_in(key_of[13], 71), 0)
    v_heads = scatter_about(key_of[2], (TOK_A, KV * HD), 1.0, 6.0, ((0, 8), (1, 4)))
    sink_logits = jnp.clip(1.0 + 4.0 * jax.random.uniform(key_of[3], (HEADS,), jnp.float32) ** block_levels(key_of[3], (HEADS,), ((0, 4),), -0.2, 0.2), 1.0, 5.0)
    out_weight = scatter_about(key_of[4], (HEADS * HD, D), HEADS ** -0.5, 1.5, ((1, 4),))
    tokens_b = scatter_about(key_of[5], (TOK_B, D), 1.0, 6.0, ((0, 8),))
    moe_gain = jnp.clip(1.0 + 0.18 * jax.random.normal(key_of[6], (D,), jnp.float32), 0.1, 1.9)
    router_group = scatter_about(key_of[7], (D, GROUPS), D ** -0.5, 0.125)
    router_expert = scatter_about(key_of[8], (D, EXPERTS), D ** -0.5, 0.125)
    route_expert = draw_route_expert(jax.random.fold_in(key_of[13], 71), 0)
    expert_gate = scatter_about(key_of[10], (EXPERTS, D, FF), D ** -0.5, 0.125, ((0, 8), (2, 4)))
    expert_up = scatter_about(key_of[11], (EXPERTS, D, FF), D ** -0.5, 0.125, ((0, 8), (2, 4)))
    expert_down = scatter_about(key_of[12], (EXPERTS, FF, D), (FF // 16) ** -0.5, 0.75, ((0, 8), (1, 4)))
    return {"q_heads": q_heads, "k_heads": k_heads, "v_heads": v_heads, "sink_logits": sink_logits, "out_weight": out_weight, "tokens_b": tokens_b, "moe_gain": moe_gain, "router_group": router_group, "router_expert": router_expert, "route_expert": route_expert, "expert_gate": expert_gate, "expert_up": expert_up, "expert_down": expert_down}


def banded(values, blocks, span_len):
    shaped = values.reshape(TOK_A, KV, HD)
    padded = jnp.concatenate([jnp.zeros((span_len, KV, HD), shaped.dtype), shaped], axis=0)
    padded = padded.reshape(blocks + 1, span_len, KV, HD)
    band = jnp.concatenate([padded[:-1], padded[1:]], axis=1)
    return jnp.moveaxis(band, 2, 0)

def gate_weights(normed, routes, router_group, router_expert):
    group_logits = jnp.dot(normed, router_group, preferred_element_type=jnp.float32)
    expert_logits = jnp.dot(normed, router_expert, preferred_element_type=jnp.float32)
    group_count = router_group.shape[1]
    expert_count = router_expert.shape[1]
    chosen_group = routes[:, 0] // (expert_count // group_count)
    group_match = chosen_group[:, None] == jnp.arange(group_count, dtype=jnp.int32)[None, :]
    group_share = lax.optimization_barrier(jnp.sum(jnp.where(group_match, jax.nn.softmax(group_logits, axis=-1), 0.0), axis=-1))
    expert_match = routes[:, :, None] == jnp.arange(expert_count, dtype=jnp.int32)[None, None, :]
    picked = lax.optimization_barrier(jnp.sum(jnp.where(expert_match, expert_logits[:, None, :], 0.0), axis=-1))
    return group_share[:, None] * jax.nn.softmax(picked, axis=-1)

def reference(q_heads, k_heads, v_heads, sink_logits, out_weight, tokens_b, moe_gain, router_group, router_expert, route_expert, expert_gate, expert_up, expert_down):
    span_len = WINDOW
    blocks = TOK_A // span_len
    group_size = HEADS // KV
    query_blocks = jnp.moveaxis(q_heads.reshape(blocks, span_len, KV, group_size, HD), 2, 0)
    key_band = banded(k_heads, blocks, span_len)
    value_band = banded(v_heads, blocks, span_len)
    query_index = jnp.arange(span_len, dtype=jnp.int32)[:, None]
    key_index = jnp.arange(2 * span_len, dtype=jnp.int32)[None, :]
    distance = query_index + span_len - key_index
    key_place = jnp.arange(blocks, dtype=jnp.int32)[:, None, None] * span_len + key_index[None] - span_len
    allowed = (distance >= 0)[None] & (distance < span_len)[None] & (key_place >= 0)
    sink_rows = sink_logits.reshape(KV, group_size)

    def one_head(packed):
        query_block, key_rows, value_rows, sink_row = packed
        scores = jnp.einsum('nqgd,nkd->ngqk', query_block.astype(jnp.float32), key_rows.astype(jnp.float32)) * HD ** (-0.5)
        masked = jnp.where(allowed[:, None], scores, -1e+30)
        sink_full = sink_row[None, :, None]
        row_max = jnp.maximum(lax.optimization_barrier(jnp.max(masked, axis=-1)), sink_full)
        weights_exp = jnp.exp(masked - row_max[..., None])
        denominator = lax.optimization_barrier(jnp.sum(weights_exp, axis=-1)) + jnp.exp(sink_full - row_max)
        probs = lax.optimization_barrier((weights_exp / denominator[..., None]).astype(jnp.bfloat16))
        mixed = jnp.einsum('ngqk,nkd->nqgd', probs.astype(jnp.float32), value_rows.astype(jnp.float32))
        return mixed.astype(jnp.bfloat16)
    attended = lax.map(one_head, (query_blocks, key_band, value_band, sink_rows))
    attended = jnp.moveaxis(attended, 0, 2).reshape(TOK_A, HEADS * HD)
    mixer_out = jnp.dot(attended, out_weight, preferred_element_type=jnp.float32).astype(jnp.bfloat16)
    blocks_b = N_EP * N_TP
    values = tokens_b.astype(jnp.float32)
    normed = (values * lax.rsqrt(lax.optimization_barrier(jnp.mean(values * values, axis=-1, keepdims=True)) + 1e-06) * moe_gain).astype(jnp.bfloat16)
    gates = gate_weights(normed, route_expert, router_group, router_expert)
    flat_routes = route_expert.reshape(blocks_b, 2 * ROW_B)
    onehot = (flat_routes[:, :, None] == jnp.arange(EXPERTS, dtype=jnp.int32)[None, None, :]).astype(jnp.int32)
    places = lax.optimization_barrier(jnp.sum(onehot * jnp.cumsum(onehot, axis=1), axis=2)) - 1
    token_ids = (jnp.arange(TOK_B * 2, dtype=jnp.int32) // 2).reshape(blocks_b, 2 * ROW_B)
    block_ids = jnp.broadcast_to(jnp.arange(blocks_b, dtype=jnp.int32)[:, None], (blocks_b, 2 * ROW_B))
    slot_token = jnp.full((EXPERTS, blocks_b, CAP), TOK_B, jnp.int32).at[flat_routes, block_ids, places].set(token_ids)
    slot_gate = jnp.zeros((EXPERTS, blocks_b, CAP), jnp.float32).at[flat_routes, block_ids, places].set(gates.reshape(blocks_b, 2 * ROW_B))
    padded_rows = jnp.concatenate([normed, jnp.zeros((1, D), jnp.bfloat16)], axis=0)
    hidden_block = FF // N_TP

    def one_expert(running, packed):
        token_list, gate_list, w_gate, w_up, w_down = packed
        rows_in = padded_rows[token_list]
        gate_pre = jnp.dot(rows_in, w_gate, preferred_element_type=jnp.float32)
        up_pre = jnp.dot(rows_in, w_up, preferred_element_type=jnp.float32)
        activated = lax.optimization_barrier((jax.nn.silu(gate_pre) * up_pre).astype(jnp.bfloat16))
        pieces = jnp.einsum('ntf,tfd->ntd', activated.reshape(-1, N_TP, hidden_block).astype(jnp.float32), w_down.reshape(N_TP, hidden_block, D).astype(jnp.float32))
        pieces = lax.optimization_barrier(pieces.astype(jnp.bfloat16)).astype(jnp.float32)
        expert_out = lax.optimization_barrier(lax.optimization_barrier(jnp.sum(pieces, axis=1)).astype(jnp.bfloat16)).astype(jnp.float32)
        running = running.at[token_list].add(gate_list[:, None] * expert_out)
        return (running, None)
    running = jnp.zeros((TOK_B + 1, D), jnp.float32)
    running, _ = lax.scan(one_expert, running, (slot_token.reshape(EXPERTS, -1), slot_gate.reshape(EXPERTS, -1), expert_gate, expert_up, expert_down))
    moe_out = running[:TOK_B].astype(jnp.bfloat16)
    return (mixer_out, moe_out)
```

```python
import functools

import jax
import jax.numpy as jnp
from jax import lax
from jax.experimental import pallas as pl
from jax.experimental.pallas import tpu as pltpu
from jax.sharding import PartitionSpec as P

HEADS = 16
KV = 4
HD = 64
WINDOW = 128


def shifted(value, axis, steps):
    count = lax.axis_size(axis)
    leading, last = (max(0, -steps), min(count, count - steps))
    return lax.ppermute(value, axis, [(source, source + steps) for source in range(leading, last)])


def normalize(rows_in, gain):
    values = rows_in.astype(jnp.float32)
    scaled = values * lax.rsqrt(jnp.mean(values * values, axis=-1, keepdims=True) + 1e-06) * gain
    return scaled.astype(jnp.bfloat16)


def gate_weights(normed, routes, router_group, router_expert):
    group_logits = jnp.dot(normed, router_group, preferred_element_type=jnp.float32)
    expert_logits = jnp.dot(normed, router_expert, preferred_element_type=jnp.float32)
    group_count = router_group.shape[1]
    expert_count = router_expert.shape[1]
    chosen_group = routes[:, 0] // (expert_count // group_count)
    group_match = chosen_group[:, None] == jnp.arange(group_count, dtype=jnp.int32)[None, :]
    group_share = jnp.sum(
        jnp.where(group_match, jax.nn.softmax(group_logits, axis=-1), 0.0), axis=-1
    )
    expert_match = routes[:, :, None] == jnp.arange(expert_count, dtype=jnp.int32)[None, None, :]
    picked = jnp.sum(jnp.where(expert_match, expert_logits[:, None, :], 0.0), axis=-1)
    return group_share[:, None] * jax.nn.softmax(picked, axis=-1)


def slot_positions(routes, sub_count, expert_count):
    flat_routes = routes.reshape(sub_count, -1)
    onehot = (
        flat_routes[:, :, None] == jnp.arange(expert_count, dtype=jnp.int32)[None, None, :]
    ).astype(jnp.int32)
    places = jnp.sum(onehot * jnp.cumsum(onehot, axis=1), axis=2) - 1
    return (flat_routes, places)


def fill_slots(normed, flat_routes, places, sub_count, expert_count, capacity, exp_local):
    sub_index = jnp.arange(sub_count, dtype=jnp.int32)[:, None]
    target = ((flat_routes * sub_count + sub_index) * capacity + places).reshape(-1)
    source = jnp.repeat(normed, 2, axis=0)
    buffer = jnp.zeros((expert_count * sub_count * capacity, normed.shape[1]), jnp.bfloat16)
    buffer = buffer.at[target].set(source)
    return buffer.reshape(
        expert_count // exp_local, exp_local, sub_count, capacity, normed.shape[1]
    )


LANES = 128
MESH = pl.DeviceIdType.MESH


def moe_kernel(
    groups,
    xs_ref,
    gate_hbm,
    up_hbm,
    down_hbm,
    out_ref,
    rows,
    part,
    wg,
    wu,
    wd,
    act,
    from_core,
    relay_x,
    relay_y,
    from_x,
    from_y,
    total,
    back,
    load_sem,
    send_sem,
    recv_sem,
):
    ep, tp = lax.axis_index("ep"), lax.axis_index("tp")
    group, member = ep // 2, ep % 2
    x, core = tp // 2, tp % 2
    tp_x, tp_c = (1 - x) * 2 + core, x * 2 + (1 - core)
    ep_y = group * 2 + (1 - member)
    x_dev, y_dev, c_dev = (ep, tp_x), (ep_y, tp), (ep, tp_c)
    width = xs_ref.shape[1]
    block = xs_ref.shape[0]
    depth = out_ref.shape[1]
    chunk = block // groups
    half = block // 2
    hidden = wg.shape[2]
    lo, hi = pl.ds(0, half), pl.ds(half, half)
    own = member * 4 + tp
    slot_x = member * 4 + tp_x
    slot_y = (1 - member) * 4 + tp
    slot_d = (1 - member) * 4 + tp_x
    mate = 1 - 2 * core

    loads = [
        pltpu.make_async_copy(source, held, load_sem.at[i])
        for i, (source, held) in enumerate(((gate_hbm, wg), (up_hbm, wu), (down_hbm, wd)))
    ]
    for load in loads:
        load.start()

    planes = [((group + step) % groups) for step in range(1, groups)]
    barrier = pltpu.get_barrier_semaphore()
    peers = [(plane * 2 + member, tp) for plane in planes] + [x_dev, y_dev, c_dev]
    for peer in peers:
        pl.semaphore_signal(barrier, inc=1, device_id=peer, device_id_type=MESH)
    pl.semaphore_wait(barrier, len(peers))

    started = []

    def send(index, source, target, device):
        copy = pltpu.make_async_remote_copy(
            src_ref=source,
            dst_ref=target,
            send_sem=send_sem.at[index],
            recv_sem=recv_sem.at[index],
            device_id=device,
            device_id_type=MESH,
        )
        copy.start()
        started.append(copy)
        return copy

    my_chunk = pl.ds(pl.multiple_of(group * chunk, chunk), chunk)
    keep = pltpu.make_async_copy(xs_ref.at[my_chunk], rows.at[own, my_chunk], load_sem.at[3])
    keep.start()
    z_out = []
    for step, plane in enumerate(planes):
        there = pl.ds(pl.multiple_of(plane * chunk, chunk), chunk)
        z_out.append(
            send(step, xs_ref.at[there], rows.at[own, my_chunk], (plane * 2 + member, tp))
        )
    keep.wait()
    for copy in z_out:
        copy.wait_recv()

    base = groups - 1
    own_c = send(base, rows.at[own], rows.at[own], c_dev)
    x_lo = send(base + 1, rows.at[own, lo], rows.at[own, lo], x_dev)
    y_hi = send(base + 2, rows.at[own, hi], rows.at[own, hi], y_dev)
    x_hi = send(base + 3, rows.at[own, hi], rows.at[own, hi], x_dev)
    y_lo = send(base + 4, rows.at[own, lo], rows.at[own, lo], y_dev)
    for load in loads:
        load.wait()

    def experts(slot):
        first = slot - core
        batch = 2 * block
        pair = pl.ds(first, 2)

        tokens = rows[pair, :, :depth].reshape(batch, depth)
        shares = rows[pair, :, depth:].reshape(batch, LANES).astype(jnp.float32)
        lane = lax.broadcasted_iota(jnp.int32, shares.shape, 1) % (LANES // 2)

        def one(e, carry):
            share = jnp.sum(
                jnp.where(lane == member * wg.shape[0] + e, shares, 0.0), axis=1, keepdims=True
            )
            pre = jnp.dot(tokens, wg[e], preferred_element_type=jnp.float32)
            up = jnp.dot(tokens, wu[e], preferred_element_type=jnp.float32)
            act[e] = (jax.nn.silu(pre) * up * share).astype(jnp.bfloat16)
            return carry

        lax.fori_loop(0, wg.shape[0], one, 0)
        acts = jnp.concatenate([act[e] for e in range(wg.shape[0])], axis=1)
        tile = 512

        def column(n, carry):
            columns = pl.ds(pl.multiple_of(n * tile, tile), tile)
            value = jnp.dot(acts, wd[:, columns], preferred_element_type=jnp.float32)
            part[pair, :, columns] = value.astype(jnp.bfloat16).reshape(2, block, tile)
            return carry

        lax.fori_loop(0, depth // tile, column, 0)

    own_c.wait_recv()
    experts(own)
    give = base + 5
    sum_own = send(give, part.at[own + mate], from_core.at[0], c_dev)

    x_lo.wait_recv()
    relay_to_y = send(give + 1, rows.at[slot_x, lo], rows.at[slot_x, lo], y_dev)
    y_hi.wait_recv()
    relay_to_x = send(give + 2, rows.at[slot_y, hi], rows.at[slot_y, hi], x_dev)
    x_hi.wait_recv()
    x_core = send(give + 3, rows.at[slot_x], rows.at[slot_x], c_dev)
    y_lo.wait_recv()
    y_core = send(give + 4, rows.at[slot_y], rows.at[slot_y], c_dev)

    x_core.wait_recv()
    experts(slot_x)
    sum_x = send(give + 5, part.at[slot_x + mate], from_core.at[1], c_dev)
    y_core.wait_recv()
    experts(slot_y)
    sum_y = send(give + 6, part.at[slot_y + mate], from_core.at[2], c_dev)

    relay_to_y.wait_recv()
    relay_to_x.wait_recv()
    d_core = send(give + 7, rows.at[slot_d], rows.at[slot_d], c_dev)

    def add(target, index, other, other_index):
        target[index] = (
            target[index].astype(jnp.float32) + other[other_index].astype(jnp.float32)
        ).astype(jnp.bfloat16)

    sum_x.wait_recv()
    add(part, slot_x, from_core, 1)
    back_x_hi = send(give + 8, part.at[slot_x, hi], from_x.at[hi], x_dev)
    sum_y.wait_recv()
    add(part, slot_y, from_core, 2)
    back_y_lo = send(give + 9, part.at[slot_y, lo], from_y.at[lo], y_dev)

    d_core.wait_recv()
    experts(slot_d)
    sum_d = send(give + 10, part.at[slot_d + mate], from_core.at[3], c_dev)
    sum_d.wait_recv()
    add(part, slot_d, from_core, 3)
    diag_y = send(give + 11, part.at[slot_d, lo], relay_y, y_dev)
    diag_x = send(give + 12, part.at[slot_d, hi], relay_x, x_dev)
    sum_own.wait_recv()
    add(part, own, from_core, 0)
    diag_y.wait_recv()
    add(part, (slot_x, lo), relay_y, ...)
    back_x_lo = send(give + 13, part.at[slot_x, lo], from_x.at[lo], x_dev)
    diag_x.wait_recv()
    add(part, (slot_y, hi), relay_x, ...)
    back_y_hi = send(give + 14, part.at[slot_y, hi], from_y.at[hi], y_dev)
    for copy in (back_x_hi, back_y_lo, back_x_lo, back_y_hi):
        copy.wait_recv()
    total[...] = (
        part[own].astype(jnp.float32)
        + from_x[...].astype(jnp.float32)
        + from_y[...].astype(jnp.float32)
    ).astype(jnp.bfloat16)

    last = give + 15
    home = []
    for step, plane in enumerate(planes):
        there = pl.ds(pl.multiple_of(plane * chunk, chunk), chunk)
        home.append(
            send(last + step, total.at[there], back.at[my_chunk], (plane * 2 + member, tp))
        )
    stay = pltpu.make_async_copy(total.at[my_chunk], back.at[my_chunk], load_sem.at[3])
    stay.start()
    stay.wait()
    for copy in home:
        copy.wait_recv()
    out_ref[...] = back[...]
    for copy in started:
        copy.wait_send()


def moe_exchange(sorted_rows, expert_gate, expert_up, expert_down, groups):
    block, width = sorted_rows.shape
    experts, depth, hidden = expert_gate.shape
    down = expert_down.reshape(experts * hidden, depth)
    copies = 2 * (groups - 1) + 20
    bf16 = jnp.bfloat16
    anywhere = pl.BlockSpec(memory_space=pl.ANY)
    vmem = pl.BlockSpec(memory_space=pltpu.VMEM)
    return pl.pallas_call(
        functools.partial(moe_kernel, groups),
        out_shape=jax.ShapeDtypeStruct((block, depth), bf16),
        in_specs=[vmem, anywhere, anywhere, anywhere],
        out_specs=vmem,
        scratch_shapes=[
            pltpu.VMEM((8, block, width), bf16),
            pltpu.VMEM((8, block, depth), bf16),
            pltpu.VMEM(expert_gate.shape, bf16),
            pltpu.VMEM(expert_up.shape, bf16),
            pltpu.VMEM(down.shape, bf16),
            pltpu.VMEM((experts, 2 * block, hidden), bf16),
            pltpu.VMEM((4, block, depth), bf16),
            pltpu.VMEM((block // 2, depth), bf16),
            pltpu.VMEM((block // 2, depth), bf16),
            pltpu.VMEM((block, depth), bf16),
            pltpu.VMEM((block, depth), bf16),
            pltpu.VMEM((block, depth), bf16),
            pltpu.VMEM((block, depth), bf16),
            pltpu.SemaphoreType.DMA((4,)),
            pltpu.SemaphoreType.DMA((copies,)),
            pltpu.SemaphoreType.DMA((copies,)),
        ],
        cost_estimate=pl.CostEstimate(
            flops=60_000_000_000, bytes_accessed=200_000_000, transcendentals=0
        ),
        compiler_params=pltpu.CompilerParams(
            collective_id=0, has_side_effects=True, vmem_limit_bytes=48 * 2**20
        ),
    )(sorted_rows, expert_gate, expert_up, down)


def moe_by_group(
    tokens_b,
    moe_gain,
    router_group,
    router_expert,
    route_expert,
    expert_gate,
    expert_up,
    expert_down,
):
    tp_count = lax.axis_size("tp")
    tp_index = lax.axis_index("tp")
    groups = router_group.shape[1]
    group_experts = router_expert.shape[1] // groups
    rows_dev = tokens_b.shape[0] // tp_count
    routes = lax.dynamic_slice_in_dim(route_expert, tp_index * rows_dev, rows_dev, 0)
    normed = normalize(
        lax.dynamic_slice_in_dim(tokens_b, tp_index * rows_dev, rows_dev, 0), moe_gain
    )
    gates = gate_weights(normed, routes, router_group, router_expert)
    lanes = jnp.arange(LANES // 2, dtype=jnp.int32)
    share = jnp.sum(
        jnp.where((routes % group_experts)[:, :, None] == lanes, gates[:, :, None], 0.0), axis=1
    )
    coarse = lax.reduce_precision(share, 8, 7)
    extended = jnp.concatenate(
        [normed, coarse.astype(jnp.bfloat16), (share - coarse).astype(jnp.bfloat16)], axis=1
    )
    named = routes[:, 0] // group_experts
    same = named[:, None] == named[None, :]
    order = jnp.arange(rows_dev, dtype=jnp.int32)
    rank = jnp.sum((same & (order[None, :] < order[:, None])).astype(jnp.int32), axis=1)
    place = named * (rows_dev // groups) + rank
    take = (place[None, :] == order[:, None]).astype(jnp.bfloat16)
    put = (place[:, None] == order[None, :]).astype(jnp.bfloat16)
    sorted_rows = jnp.dot(take, extended, preferred_element_type=jnp.float32)
    result = moe_exchange(
        sorted_rows.astype(jnp.bfloat16), expert_gate, expert_up, expert_down, groups
    )
    return jnp.dot(put, result, preferred_element_type=jnp.float32).astype(jnp.bfloat16)


def per_device(
    q_heads,
    k_heads,
    v_heads,
    sink_logits,
    out_weight,
    tokens_b,
    moe_gain,
    router_group,
    router_expert,
    route_expert,
    expert_gate,
    expert_up,
    expert_down,
):
    span_len = WINDOW
    row_count = q_heads.shape[0]
    kv_local = k_heads.shape[1] // HD
    group_size = HEADS // KV
    blocks = row_count // span_len
    stacked = jnp.stack([k_heads[row_count - span_len :], v_heads[row_count - span_len :]])
    earlier = shifted(stacked, "ep", 1)

    def make_band(own_rows, prev_rows):
        extended = jnp.concatenate([prev_rows, own_rows], axis=0).reshape(
            blocks + 1, span_len, kv_local, HD
        )
        return jnp.concatenate([extended[:-1], extended[1:]], axis=1)

    key_band = make_band(k_heads, earlier[0])
    value_band = make_band(v_heads, earlier[1])
    query_blocks = q_heads.reshape(blocks, span_len, kv_local, group_size, HD)
    scores = jnp.einsum(
        "nqhgd,nkhd->nhgqk", query_blocks, key_band, preferred_element_type=jnp.float32
    ) * HD ** (-0.5)
    first_row = lax.axis_index("ep") * row_count
    query_index = jnp.arange(span_len, dtype=jnp.int32)[:, None]
    key_index = jnp.arange(2 * span_len, dtype=jnp.int32)[None, :]
    distance = query_index + span_len - key_index
    key_place = (
        first_row
        + jnp.arange(blocks, dtype=jnp.int32)[:, None, None] * span_len
        + key_index[None]
        - span_len
    )
    allowed = (distance >= 0)[None] & (distance < span_len)[None] & (key_place >= 0)
    masked = jnp.where(allowed[:, None, None], scores, -1e30)
    sink_full = sink_logits.reshape(kv_local, group_size)[None, :, :, None]
    row_max = jnp.maximum(jnp.max(masked, axis=-1), sink_full)
    weights_exp = jnp.exp(masked - row_max[..., None])
    denominator = jnp.sum(weights_exp, axis=-1) + jnp.exp(sink_full - row_max)
    probs = (weights_exp / denominator[..., None]).astype(jnp.bfloat16)
    attended = jnp.einsum(
        "nhgqk,nkhd->nqhgd", probs, value_band, preferred_element_type=jnp.float32
    )
    attended = attended.astype(jnp.bfloat16).reshape(row_count, kv_local * group_size * HD)
    mixed = jnp.dot(
        lax.all_gather(attended, "tp", axis=1, tiled=True),
        out_weight,
        preferred_element_type=jnp.float32,
    )
    mixer_out = mixed.astype(jnp.bfloat16)
    groups = router_group.shape[1]
    if lax.axis_size("ep") == 2 * groups and lax.axis_size("tp") == 4:
        moe_out = moe_by_group(
            tokens_b,
            moe_gain,
            router_group,
            router_expert,
            route_expert,
            expert_gate,
            expert_up,
            expert_down,
        )
        return (mixer_out, moe_out)
    tp_count = lax.axis_size("tp")
    tp_index = lax.axis_index("tp")
    exp_local = expert_gate.shape[0]
    expert_count = exp_local * lax.axis_size("ep")
    rows_dev = tokens_b.shape[0] // tp_count
    capacity = min(4 * rows_dev // expert_count, rows_dev // 4)
    own_routes = lax.dynamic_slice_in_dim(route_expert, tp_index * rows_dev, rows_dev, 0)
    own_normed = normalize(
        lax.dynamic_slice_in_dim(tokens_b, tp_index * rows_dev, rows_dev, 0), moe_gain
    )
    flat_routes, places = slot_positions(own_routes, 1, expert_count)
    buffer = fill_slots(own_normed, flat_routes, places, 1, expert_count, capacity, exp_local)
    delivered = lax.all_to_all(buffer, "ep", split_axis=0, concat_axis=0, tiled=True)
    arrived = lax.all_gather(delivered, "tp", axis=2, tiled=True)
    own_flat = flat_routes[0]
    own_places = places[0]
    gates = gate_weights(own_normed, own_routes, router_group, router_expert)
    gate_pre = jnp.einsum(
        "setcd,edf->setcf", arrived, expert_gate, preferred_element_type=jnp.float32
    )
    up_pre = jnp.einsum("setcd,edf->setcf", arrived, expert_up, preferred_element_type=jnp.float32)
    activated = (jax.nn.silu(gate_pre) * up_pre).astype(jnp.bfloat16)
    partial_value = jnp.einsum(
        "setcf,efd->setcd", activated, expert_down, preferred_element_type=jnp.float32
    )
    summed = lax.psum_scatter(
        partial_value.astype(jnp.bfloat16), "tp", scatter_dimension=2, tiled=True
    )
    returned = lax.all_to_all(summed, "ep", split_axis=0, concat_axis=0, tiled=True)
    returned = returned.reshape(expert_count * capacity, returned.shape[-1])
    picked_rows = returned[own_flat * capacity + own_places].reshape(
        rows_dev, 2, returned.shape[-1]
    )
    moe_out = jnp.sum(gates[:, :, None] * picked_rows.astype(jnp.float32), axis=1).astype(
        jnp.bfloat16
    )
    return (mixer_out, moe_out)


def solution(mesh):
    in_specs = (
        P("ep", "tp"),
        P("ep", "tp"),
        P("ep", "tp"),
        P("tp"),
        P(None, "tp"),
        P("ep", None),
        P(),
        P(),
        P(),
        P("ep", None),
        P("ep", None, "tp"),
        P("ep", None, "tp"),
        P("ep", "tp", None),
    )
    out_specs = (P("ep", "tp"), P(("ep", "tp"), None))
    return jax.shard_map(
        per_device, mesh=mesh, in_specs=in_specs, out_specs=out_specs, check_vma=False
    )
```

```python
import functools

import jax
import jax.numpy as jnp
from jax import lax
from jax.experimental import pallas as pl
from jax.experimental.pallas import tpu as pltpu
from jax.sharding import PartitionSpec as P

HEADS = 16
KV = 4
HD = 64
WINDOW = 128


def shifted(value, axis, steps):
    count = lax.axis_size(axis)
    leading, last = (max(0, -steps), min(count, count - steps))
    return lax.ppermute(value, axis, [(source, source + steps) for source in range(leading, last)])


def normalize(rows_in, gain):
    values = rows_in.astype(jnp.float32)
    scaled = values * lax.rsqrt(jnp.mean(values * values, axis=-1, keepdims=True) + 1e-06) * gain
    return scaled.astype(jnp.bfloat16)


def gate_weights(normed, routes, router_group, router_expert):
    group_logits = jnp.dot(normed, router_group, preferred_element_type=jnp.float32)
    expert_logits = jnp.dot(normed, router_expert, preferred_element_type=jnp.float32)
    group_count = router_group.shape[1]
    expert_count = router_expert.shape[1]
    chosen_group = routes[:, 0] // (expert_count // group_count)
    group_match = chosen_group[:, None] == jnp.arange(group_count, dtype=jnp.int32)[None, :]
    group_share = jnp.sum(
        jnp.where(group_match, jax.nn.softmax(group_logits, axis=-1), 0.0), axis=-1
    )
    expert_match = routes[:, :, None] == jnp.arange(expert_count, dtype=jnp.int32)[None, None, :]
    picked = jnp.sum(jnp.where(expert_match, expert_logits[:, None, :], 0.0), axis=-1)
    return group_share[:, None] * jax.nn.softmax(picked, axis=-1)


def slot_positions(routes, sub_count, expert_count):
    flat_routes = routes.reshape(sub_count, -1)
    onehot = (
        flat_routes[:, :, None] == jnp.arange(expert_count, dtype=jnp.int32)[None, None, :]
    ).astype(jnp.int32)
    places = jnp.sum(onehot * jnp.cumsum(onehot, axis=1), axis=2) - 1
    return (flat_routes, places)


def fill_slots(normed, flat_routes, places, sub_count, expert_count, capacity, exp_local):
    sub_index = jnp.arange(sub_count, dtype=jnp.int32)[:, None]
    target = ((flat_routes * sub_count + sub_index) * capacity + places).reshape(-1)
    source = jnp.repeat(normed, 2, axis=0)
    buffer = jnp.zeros((expert_count * sub_count * capacity, normed.shape[1]), jnp.bfloat16)
    buffer = buffer.at[target].set(source)
    return buffer.reshape(
        expert_count // exp_local, exp_local, sub_count, capacity, normed.shape[1]
    )


LANES = 128
MESH = pl.DeviceIdType.MESH


def fused_kernel(
    groups,
    sink_ref,
    q_ref,
    kv_ref,
    xs_ref,
    gate_hbm,
    up_hbm,
    down_hbm,
    proj_hbm,
    mixer_ref,
    out_ref,
    kv_ext,
    heads,
    rows,
    part,
    wg,
    wu,
    wd,
    proj,
    act,
    from_core,
    relay_x,
    relay_y,
    from_x,
    from_y,
    total,
    back,
    load_sem,
    send_sem,
    recv_sem,
):
    ep, tp = lax.axis_index("ep"), lax.axis_index("tp")
    group, member = ep // 2, ep % 2
    x, core = tp // 2, tp % 2
    tp_x, tp_c = (1 - x) * 2 + core, x * 2 + (1 - core)
    ep_y = group * 2 + (1 - member)
    ep_count = groups * 2
    x_dev, y_dev, c_dev = (ep, tp_x), (ep_y, tp), (ep, tp_c)
    next_dev = ((ep + 1) % ep_count, tp)
    prev_dev = ((ep + ep_count - 1) % ep_count, tp)
    depth = out_ref.shape[1]
    chunk = xs_ref.shape[0] // groups
    half = chunk // 2
    row_count = q_ref.shape[0]
    lo, hi = pl.ds(0, half), pl.ds(half, half)
    mine, other = core * 4, (1 - core) * 4
    own = mine + member * 2 + x
    slot_x = mine + member * 2 + (1 - x)
    slot_y = mine + (1 - member) * 2 + x
    slot_d = mine + (1 - member) * 2 + (1 - x)
    mine_slots, other_slots = pl.ds(mine, 4), pl.ds(other, 4)

    pairs = ((gate_hbm, wg), (up_hbm, wu), (down_hbm, wd), (proj_hbm, proj))
    loads = [
        pltpu.make_async_copy(source, held, load_sem.at[i])
        for i, (source, held) in enumerate(pairs)
    ]
    for load in loads:
        load.start()

    barrier = pltpu.get_barrier_semaphore()
    ahead = [((group + step) % groups) * 2 + member for step in range(1, groups)]
    peers = [(plane, tp) for plane in ahead] + [x_dev, y_dev, c_dev, next_dev, prev_dev]
    for peer in peers:
        pl.semaphore_signal(barrier, inc=1, device_id=peer, device_id_type=MESH)
    pl.semaphore_wait(barrier, len(peers))

    started = []

    def send(source, target, device):
        index = len(started)
        copy = pltpu.make_async_remote_copy(
            src_ref=source,
            dst_ref=target,
            send_sem=send_sem.at[index],
            recv_sem=recv_sem.at[index],
            device_id=device,
            device_id_type=MESH,
        )
        copy.start()
        started.append(copy)
        return copy

    my_chunk = pl.ds(pl.multiple_of(group * chunk, chunk), chunk)
    keep = pltpu.make_async_copy(xs_ref.at[my_chunk], rows.at[0, own], load_sem.at[4])
    keep.start()
    halo = send(kv_ref.at[pl.ds(row_count - WINDOW, WINDOW)], kv_ext.at[pl.ds(0, WINDOW)], next_dev)
    z_out = [keep]
    for step in range(1, groups):
        plane = (group + step) % groups
        there = pl.ds(pl.multiple_of(plane * chunk, chunk), chunk)
        z_out.append(send(xs_ref.at[there], rows.at[step, own], (plane * 2 + member, tp)))
    kv_ext[pl.ds(WINDOW, row_count)] = kv_ref[...]

    held = [dict() for _ in range(groups)]

    def stage_a(s):
        if s:
            z_out[s].wait_recv()
        else:
            keep.wait()
        held[s]["x"] = send(rows.at[s, own], rows.at[s, own], x_dev)
        held[s]["y"] = send(rows.at[s, own], rows.at[s, own], y_dev)

    def stage_b(s):
        held[s]["x"].wait_recv()
        held[s]["to_y"] = send(rows.at[s, slot_x, lo], rows.at[s, slot_x, lo], y_dev)
        held[s]["y"].wait_recv()
        held[s]["to_x"] = send(rows.at[s, slot_y, hi], rows.at[s, slot_y, hi], x_dev)

    def stage_c(s):
        held[s]["to_y"].wait_recv()
        held[s]["to_x"].wait_recv()
        held[s]["core"] = send(rows.at[s, mine_slots], rows.at[s, mine_slots], c_dev)

    def stage_d(s):
        held[s]["core"].wait_recv()
        batch = 8 * chunk
        tokens = rows[s, :, :, :depth].reshape(batch, depth)
        shares = rows[s, :, :, depth:].reshape(batch, LANES).astype(jnp.float32)
        lane = lax.broadcasted_iota(jnp.int32, shares.shape, 1) % (LANES // 2)

        def one(e, carry):
            share = jnp.sum(
                jnp.where(lane == member * wg.shape[0] + e, shares, 0.0), axis=1, keepdims=True
            )
            pre = jnp.dot(tokens, wg[e], preferred_element_type=jnp.float32)
            up = jnp.dot(tokens, wu[e], preferred_element_type=jnp.float32)
            act[e] = (jax.nn.silu(pre) * up * share).astype(jnp.bfloat16)
            return carry

        lax.fori_loop(0, wg.shape[0], one, 0)
        acts = jnp.concatenate([act[e] for e in range(wg.shape[0])], axis=1)
        tile = 512

        def column(n, carry):
            columns = pl.ds(pl.multiple_of(n * tile, tile), tile)
            value = jnp.dot(acts, wd[:, columns], preferred_element_type=jnp.float32)
            part[s, :, :, columns] = value.astype(jnp.bfloat16).reshape(8, chunk, tile)
            return carry

        lax.fori_loop(0, depth // tile, column, 0)
        held[s]["sum"] = send(part.at[s, other_slots], from_core.at[s], c_dev)

    def add(index, term):
        part[index] = (part[index].astype(jnp.float32) + term.astype(jnp.float32)).astype(
            jnp.bfloat16
        )

    def stage_e(s):
        held[s]["sum"].wait_recv()
        add((s, mine_slots), from_core[s])
        held[s]["d_y"] = send(part.at[s, slot_d, lo], relay_y.at[s], y_dev)
        held[s]["d_x"] = send(part.at[s, slot_d, hi], relay_x.at[s], x_dev)
        held[s]["x_hi"] = send(part.at[s, slot_x, hi], from_x.at[s, hi], x_dev)
        held[s]["y_lo"] = send(part.at[s, slot_y, lo], from_y.at[s, lo], y_dev)

    def stage_f(s):
        held[s]["d_y"].wait_recv()
        add((s, slot_x, lo), relay_y[s])
        held[s]["x_lo"] = send(part.at[s, slot_x, lo], from_x.at[s, lo], x_dev)
        held[s]["d_x"].wait_recv()
        add((s, slot_y, hi), relay_x[s])
        held[s]["y_hi"] = send(part.at[s, slot_y, hi], from_y.at[s, hi], y_dev)

    def stage_h(s):
        for name in ("x_hi", "y_lo", "x_lo", "y_hi"):
            held[s][name].wait_recv()
        summed = (
            part[s, own].astype(jnp.float32)
            + from_x[s].astype(jnp.float32)
            + from_y[s].astype(jnp.float32)
        ).astype(jnp.bfloat16)
        if s:
            total[s] = summed
            plane = (group + groups - s) % groups
            held[s]["home"] = send(total.at[s], back.at[my_chunk], (plane * 2 + member, tp))
        else:
            back[my_chunk] = summed

    head_count = q_ref.shape[1] // HD
    query_at = lax.broadcasted_iota(jnp.int32, (WINDOW, 2 * WINDOW), 0)
    key_at = lax.broadcasted_iota(jnp.int32, (WINDOW, 2 * WINDOW), 1)
    distance = query_at + WINDOW - key_at
    near = (distance >= 0) & (distance < WINDOW)

    def attend(b, carry):
        start = pl.multiple_of(b * WINDOW, WINDOW)
        band = kv_ext[pl.ds(start, 2 * WINDOW)]
        queries = q_ref[pl.ds(start, WINDOW)]
        keys = band[:, :HD]
        allowed = near & (key_at + (ep * row_count + b * WINDOW - WINDOW) >= 0)
        outs = []
        for h in range(head_count):
            query = queries[:, h * HD : (h + 1) * HD]
            scores = lax.dot_general(
                query, keys, (((1,), (1,)), ((), ())), preferred_element_type=jnp.float32
            ) * HD ** (-0.5)
            masked = jnp.where(allowed, scores, -1e30)
            sink = jnp.full((WINDOW, 1), sink_ref[h], jnp.float32)
            row_max = jnp.maximum(jnp.max(masked, axis=1, keepdims=True), sink)
            weights = jnp.exp(masked - row_max)
            denominator = jnp.sum(weights, axis=1, keepdims=True) + jnp.exp(sink - row_max)
            probs = (weights * (1.0 / denominator)).astype(jnp.bfloat16)
            both = jnp.dot(probs, band, preferred_element_type=jnp.float32)
            outs.append(both[:, HD:])
        heads[tp, pl.ds(start, WINDOW)] = jnp.concatenate(outs, axis=1).astype(jnp.bfloat16)
        return carry

    blocks = row_count // WINDOW
    piece = row_count // 4
    att_x = []

    def send_heads(i):
        span = pl.ds(i * piece, piece)
        att_x.append(send(heads.at[tp, span], heads.at[tp, span], x_dev))

    stage_a(0)
    lax.fori_loop(1, blocks // 2, attend, 0)
    stage_b(0)
    stage_a(1)
    lax.fori_loop(blocks // 2, blocks, attend, 0)
    stage_c(0)
    stage_b(1)
    stage_a(2)
    halo.wait_recv()
    lax.fori_loop(0, 1, attend, 0)
    send_heads(0)
    att_c = send(heads.at[tp], heads.at[tp], c_dev)
    for load in loads:
        load.wait()
    stage_d(0)
    stage_c(1)
    stage_b(2)
    stage_a(3)
    stage_e(0)
    stage_d(1)
    send_heads(1)
    stage_f(0)
    stage_c(2)
    stage_b(3)
    stage_e(1)
    stage_d(2)
    stage_h(0)
    send_heads(2)
    stage_f(1)
    stage_c(3)
    stage_e(2)
    stage_d(3)
    stage_h(1)
    stage_f(2)
    stage_e(3)
    send_heads(3)
    stage_h(2)
    stage_f(3)
    for copy in att_x:
        copy.wait_recv()
    att_cx = send(heads.at[tp_x], heads.at[tp_x], c_dev)
    att_c.wait_recv()
    att_cx.wait_recv()
    stage_h(3)

    def project(i, carry):
        span = pl.ds(pl.multiple_of(i * piece, piece), piece)
        joined = jnp.concatenate([heads[t, span] for t in range(4)], axis=1)
        mixer_ref[span] = jnp.dot(joined, proj[...], preferred_element_type=jnp.float32).astype(
            jnp.bfloat16
        )
        return carry

    lax.fori_loop(0, 4, project, 0)
    for s in range(1, groups):
        held[s]["home"].wait_recv()
    out_ref[...] = back[...]
    for copy in started:
        copy.wait_send()


def fused(sinks, q_heads, kv, sorted_rows, expert_gate, expert_up, expert_down, proj, groups):
    block, width = sorted_rows.shape
    experts, depth, hidden = expert_gate.shape
    row_count, head_width = q_heads.shape
    down = expert_down.reshape(experts * hidden, depth)
    chunk = block // groups
    copies = 14 * groups + 8
    bf16 = jnp.bfloat16
    anywhere = pl.BlockSpec(memory_space=pl.ANY)
    vmem = pl.BlockSpec(memory_space=pltpu.VMEM)
    return pl.pallas_call(
        functools.partial(fused_kernel, groups),
        out_shape=(
            jax.ShapeDtypeStruct((row_count, proj.shape[1]), bf16),
            jax.ShapeDtypeStruct((block, depth), bf16),
        ),
        in_specs=[pl.BlockSpec(memory_space=pltpu.SMEM), vmem, vmem, vmem] + [anywhere] * 4,
        out_specs=(vmem, vmem),
        scratch_shapes=[
            pltpu.VMEM((row_count + WINDOW, 2 * HD), bf16),
            pltpu.VMEM((4, row_count, head_width), bf16),
            pltpu.VMEM((groups, 8, chunk, width), bf16),
            pltpu.VMEM((groups, 8, chunk, depth), bf16),
            pltpu.VMEM(expert_gate.shape, bf16),
            pltpu.VMEM(expert_up.shape, bf16),
            pltpu.VMEM(down.shape, bf16),
            pltpu.VMEM(proj.shape, bf16),
            pltpu.VMEM((experts, 8 * chunk, hidden), bf16),
            pltpu.VMEM((groups, 4, chunk, depth), bf16),
            pltpu.VMEM((groups, chunk // 2, depth), bf16),
            pltpu.VMEM((groups, chunk // 2, depth), bf16),
            pltpu.VMEM((groups, chunk, depth), bf16),
            pltpu.VMEM((groups, chunk, depth), bf16),
            pltpu.VMEM((groups, chunk, depth), bf16),
            pltpu.VMEM((block, depth), bf16),
            pltpu.SemaphoreType.DMA((5,)),
            pltpu.SemaphoreType.DMA((copies,)),
            pltpu.SemaphoreType.DMA((copies,)),
        ],
        cost_estimate=pl.CostEstimate(
            flops=20_000_000_000, bytes_accessed=20_000_000, transcendentals=0
        ),
        compiler_params=pltpu.CompilerParams(
            collective_id=0, has_side_effects=True, vmem_limit_bytes=56 * 2**20
        ),
    )(sinks, q_heads, kv, sorted_rows, expert_gate, expert_up, down, proj)


def by_group(
    q_heads,
    k_heads,
    v_heads,
    sink_logits,
    out_weight,
    tokens_b,
    moe_gain,
    router_group,
    router_expert,
    route_expert,
    expert_gate,
    expert_up,
    expert_down,
):
    tp_count = lax.axis_size("tp")
    tp_index = lax.axis_index("tp")
    groups = router_group.shape[1]
    group_experts = router_expert.shape[1] // groups
    rows_dev = tokens_b.shape[0] // tp_count
    routes = lax.dynamic_slice_in_dim(route_expert, tp_index * rows_dev, rows_dev, 0)
    normed = normalize(
        lax.dynamic_slice_in_dim(tokens_b, tp_index * rows_dev, rows_dev, 0), moe_gain
    )
    gates = gate_weights(normed, routes, router_group, router_expert)
    lanes = jnp.arange(LANES // 2, dtype=jnp.int32)
    share = jnp.sum(
        jnp.where((routes % group_experts)[:, :, None] == lanes, gates[:, :, None], 0.0), axis=1
    )
    coarse = lax.reduce_precision(share, 8, 7)
    extended = jnp.concatenate(
        [normed, coarse.astype(jnp.bfloat16), (share - coarse).astype(jnp.bfloat16)], axis=1
    )
    named = routes[:, 0] // group_experts
    same = named[:, None] == named[None, :]
    order = jnp.arange(rows_dev, dtype=jnp.int32)
    rank = jnp.sum((same & (order[None, :] < order[:, None])).astype(jnp.int32), axis=1)
    place = named * (rows_dev // groups) + rank
    take = (place[None, :] == order[:, None]).astype(jnp.bfloat16)
    put = (place[:, None] == order[None, :]).astype(jnp.bfloat16)
    sorted_rows = jnp.dot(take, extended, preferred_element_type=jnp.float32)
    mixer_out, result = fused(
        sink_logits,
        q_heads,
        jnp.concatenate([k_heads, v_heads], axis=1),
        sorted_rows.astype(jnp.bfloat16),
        expert_gate,
        expert_up,
        expert_down,
        out_weight,
        groups,
    )
    moe_out = jnp.dot(put, result, preferred_element_type=jnp.float32).astype(jnp.bfloat16)
    return (mixer_out, moe_out)


def per_device(
    q_heads,
    k_heads,
    v_heads,
    sink_logits,
    out_weight,
    tokens_b,
    moe_gain,
    router_group,
    router_expert,
    route_expert,
    expert_gate,
    expert_up,
    expert_down,
):
    groups = router_group.shape[1]
    if (lax.axis_size("ep"), lax.axis_size("tp"), k_heads.shape[1]) == (2 * groups, 4, HD):
        return by_group(
            q_heads,
            k_heads,
            v_heads,
            sink_logits,
            out_weight,
            tokens_b,
            moe_gain,
            router_group,
            router_expert,
            route_expert,
            expert_gate,
            expert_up,
            expert_down,
        )
    span_len = WINDOW
    row_count = q_heads.shape[0]
    kv_local = k_heads.shape[1] // HD
    group_size = HEADS // KV
    blocks = row_count // span_len
    stacked = jnp.stack([k_heads[row_count - span_len :], v_heads[row_count - span_len :]])
    earlier = shifted(stacked, "ep", 1)

    def make_band(own_rows, prev_rows):
        extended = jnp.concatenate([prev_rows, own_rows], axis=0).reshape(
            blocks + 1, span_len, kv_local, HD
        )
        return jnp.concatenate([extended[:-1], extended[1:]], axis=1)

    key_band = make_band(k_heads, earlier[0])
    value_band = make_band(v_heads, earlier[1])
    query_blocks = q_heads.reshape(blocks, span_len, kv_local, group_size, HD)
    scores = jnp.einsum(
        "nqhgd,nkhd->nhgqk", query_blocks, key_band, preferred_element_type=jnp.float32
    ) * HD ** (-0.5)
    first_row = lax.axis_index("ep") * row_count
    query_index = jnp.arange(span_len, dtype=jnp.int32)[:, None]
    key_index = jnp.arange(2 * span_len, dtype=jnp.int32)[None, :]
    distance = query_index + span_len - key_index
    key_place = (
        first_row
        + jnp.arange(blocks, dtype=jnp.int32)[:, None, None] * span_len
        + key_index[None]
        - span_len
    )
    allowed = (distance >= 0)[None] & (distance < span_len)[None] & (key_place >= 0)
    masked = jnp.where(allowed[:, None, None], scores, -1e30)
    sink_full = sink_logits.reshape(kv_local, group_size)[None, :, :, None]
    row_max = jnp.maximum(jnp.max(masked, axis=-1), sink_full)
    weights_exp = jnp.exp(masked - row_max[..., None])
    denominator = jnp.sum(weights_exp, axis=-1) + jnp.exp(sink_full - row_max)
    probs = (weights_exp / denominator[..., None]).astype(jnp.bfloat16)
    attended = jnp.einsum(
        "nhgqk,nkhd->nqhgd", probs, value_band, preferred_element_type=jnp.float32
    )
    attended = attended.astype(jnp.bfloat16).reshape(row_count, kv_local * group_size * HD)
    mixed = jnp.dot(
        lax.all_gather(attended, "tp", axis=1, tiled=True),
        out_weight,
        preferred_element_type=jnp.float32,
    )
    mixer_out = mixed.astype(jnp.bfloat16)
    tp_count = lax.axis_size("tp")
    tp_index = lax.axis_index("tp")
    exp_local = expert_gate.shape[0]
    expert_count = exp_local * lax.axis_size("ep")
    rows_dev = tokens_b.shape[0] // tp_count
    capacity = min(4 * rows_dev // expert_count, rows_dev // 4)
    own_routes = lax.dynamic_slice_in_dim(route_expert, tp_index * rows_dev, rows_dev, 0)
    own_normed = normalize(
        lax.dynamic_slice_in_dim(tokens_b, tp_index * rows_dev, rows_dev, 0), moe_gain
    )
    flat_routes, places = slot_positions(own_routes, 1, expert_count)
    buffer = fill_slots(own_normed, flat_routes, places, 1, expert_count, capacity, exp_local)
    delivered = lax.all_to_all(buffer, "ep", split_axis=0, concat_axis=0, tiled=True)
    arrived = lax.all_gather(delivered, "tp", axis=2, tiled=True)
    own_flat = flat_routes[0]
    own_places = places[0]
    gates = gate_weights(own_normed, own_routes, router_group, router_expert)
    gate_pre = jnp.einsum(
        "setcd,edf->setcf", arrived, expert_gate, preferred_element_type=jnp.float32
    )
    up_pre = jnp.einsum("setcd,edf->setcf", arrived, expert_up, preferred_element_type=jnp.float32)
    activated = (jax.nn.silu(gate_pre) * up_pre).astype(jnp.bfloat16)
    partial_value = jnp.einsum(
        "setcf,efd->setcd", activated, expert_down, preferred_element_type=jnp.float32
    )
    summed = lax.psum_scatter(
        partial_value.astype(jnp.bfloat16), "tp", scatter_dimension=2, tiled=True
    )
    returned = lax.all_to_all(summed, "ep", split_axis=0, concat_axis=0, tiled=True)
    returned = returned.reshape(expert_count * capacity, returned.shape[-1])
    picked_rows = returned[own_flat * capacity + own_places].reshape(
        rows_dev, 2, returned.shape[-1]
    )
    moe_out = jnp.sum(gates[:, :, None] * picked_rows.astype(jnp.float32), axis=1).astype(
        jnp.bfloat16
    )
    return (mixer_out, moe_out)


def solution(mesh):
    in_specs = (
        P("ep", "tp"),
        P("ep", "tp"),
        P("ep", "tp"),
        P("tp"),
        P(None, "tp"),
        P("ep", None),
        P(),
        P(),
        P(),
        P("ep", None),
        P("ep", None, "tp"),
        P("ep", None, "tp"),
        P("ep", "tp", None),
    )
    out_specs = (P("ep", "tp"), P(("ep", "tp"), None))
    return jax.shard_map(
        per_device, mesh=mesh, in_specs=in_specs, out_specs=out_specs, check_vma=False
    )
```

```python
import functools

import jax
import jax.numpy as jnp
from jax import lax
from jax.experimental import pallas as pl
from jax.experimental.pallas import tpu as pltpu
from jax.sharding import PartitionSpec as P

HEADS = 16
KV = 4
HD = 64
WINDOW = 128


def shifted(value, axis, steps):
    count = lax.axis_size(axis)
    leading, last = (max(0, -steps), min(count, count - steps))
    return lax.ppermute(value, axis, [(source, source + steps) for source in range(leading, last)])


def normalize(rows_in, gain):
    values = rows_in.astype(jnp.float32)
    scaled = values * lax.rsqrt(jnp.mean(values * values, axis=-1, keepdims=True) + 1e-06) * gain
    return scaled.astype(jnp.bfloat16)


def gate_weights(normed, routes, router_group, router_expert):
    group_logits = jnp.dot(normed, router_group, preferred_element_type=jnp.float32)
    expert_logits = jnp.dot(normed, router_expert, preferred_element_type=jnp.float32)
    group_count = router_group.shape[1]
    expert_count = router_expert.shape[1]
    chosen_group = routes[:, 0] // (expert_count // group_count)
    group_match = chosen_group[:, None] == jnp.arange(group_count, dtype=jnp.int32)[None, :]
    group_share = jnp.sum(
        jnp.where(group_match, jax.nn.softmax(group_logits, axis=-1), 0.0), axis=-1
    )
    expert_match = routes[:, :, None] == jnp.arange(expert_count, dtype=jnp.int32)[None, None, :]
    picked = jnp.sum(jnp.where(expert_match, expert_logits[:, None, :], 0.0), axis=-1)
    return group_share[:, None] * jax.nn.softmax(picked, axis=-1)


def slot_positions(routes, sub_count, expert_count):
    flat_routes = routes.reshape(sub_count, -1)
    onehot = (
        flat_routes[:, :, None] == jnp.arange(expert_count, dtype=jnp.int32)[None, None, :]
    ).astype(jnp.int32)
    places = jnp.sum(onehot * jnp.cumsum(onehot, axis=1), axis=2) - 1
    return (flat_routes, places)


def fill_slots(normed, flat_routes, places, sub_count, expert_count, capacity, exp_local):
    sub_index = jnp.arange(sub_count, dtype=jnp.int32)[:, None]
    target = ((flat_routes * sub_count + sub_index) * capacity + places).reshape(-1)
    source = jnp.repeat(normed, 2, axis=0)
    buffer = jnp.zeros((expert_count * sub_count * capacity, normed.shape[1]), jnp.bfloat16)
    buffer = buffer.at[target].set(source)
    return buffer.reshape(
        expert_count // exp_local, exp_local, sub_count, capacity, normed.shape[1]
    )


LANES = 128
MESH = pl.DeviceIdType.MESH


def fused_kernel(
    groups,
    sink_ref,
    q_ref,
    k_ref,
    v_ref,
    gain_ref,
    group_ref,
    expert_ref,
    route_ref,
    tokens_hbm,
    gate_hbm,
    up_hbm,
    down_hbm,
    proj_hbm,
    mixer_ref,
    out_ref,
    k_ext,
    v_ext,
    tokens,
    xs_ref,
    heads,
    rows,
    part,
    wg,
    wu,
    wd,
    proj,
    act,
    from_core,
    relay_x,
    relay_y,
    from_x,
    from_y,
    total,
    back,
    load_sem,
    send_sem,
    recv_sem,
):
    ep, tp = lax.axis_index("ep"), lax.axis_index("tp")
    group, member = ep // 2, ep % 2
    x, core = tp // 2, tp % 2
    tp_x, tp_c = (1 - x) * 2 + core, x * 2 + (1 - core)
    ep_y = group * 2 + (1 - member)
    ep_count = groups * 2
    x_dev, y_dev, c_dev = (ep, tp_x), (ep_y, tp), (ep, tp_c)
    next_dev = ((ep + 1) % ep_count, tp)
    prev_dev = ((ep + ep_count - 1) % ep_count, tp)
    depth = out_ref.shape[1]
    chunk = xs_ref.shape[0] // groups
    half = chunk // 2
    row_count = q_ref.shape[0]
    lo, hi = pl.ds(0, half), pl.ds(half, half)
    mine, other = core * 4, (1 - core) * 4
    own = mine + member * 2 + x
    slot_x = mine + member * 2 + (1 - x)
    slot_y = mine + (1 - member) * 2 + x
    slot_d = mine + (1 - member) * 2 + (1 - x)
    mine_slots, other_slots = pl.ds(mine, 4), pl.ds(other, 4)

    pairs = ((gate_hbm, wg), (up_hbm, wu), (down_hbm, wd), (proj_hbm, proj))
    loads = [
        pltpu.make_async_copy(source, held, load_sem.at[i])
        for i, (source, held) in enumerate(pairs)
    ]
    block = xs_ref.shape[0]
    first = pl.multiple_of(tp * block, block)
    fetch = pltpu.make_async_copy(tokens_hbm.at[pl.ds(first, block)], tokens, load_sem.at[5])
    fetch.start()
    for load in loads:
        load.start()

    barrier = pltpu.get_barrier_semaphore()
    ahead = [((group + step) % groups) * 2 + member for step in range(1, groups)]
    peers = [(plane, tp) for plane in ahead] + [x_dev, y_dev, c_dev, next_dev, prev_dev]
    for peer in peers:
        pl.semaphore_signal(barrier, inc=1, device_id=peer, device_id_type=MESH)
    fetch.wait()
    values = tokens[...].astype(jnp.float32)
    scale = lax.rsqrt(jnp.mean(values * values, axis=1, keepdims=True) + 1e-06)
    normed = (values * scale * gain_ref[...]).astype(jnp.bfloat16)
    across = (((1,), (1,)), ((), ()))
    group_logits = lax.dot_general(
        group_ref[...], normed, across, preferred_element_type=jnp.float32
    )
    expert_logits = lax.dot_general(
        expert_ref[...], normed, across, preferred_element_type=jnp.float32
    )
    routes = route_ref[:, pl.ds(first, block)]
    route_a, route_b = routes[0:1], routes[1:2]
    group_experts = expert_ref.shape[0] // groups
    group_at = lax.broadcasted_iota(jnp.int32, (groups, block), 0)
    inside = route_a - group_at * group_experts
    named = (inside >= 0) & (inside < group_experts)
    group_exp = jnp.exp(group_logits - jnp.max(group_logits, axis=0, keepdims=True))
    group_share = jnp.sum(jnp.where(named, group_exp, 0.0), axis=0, keepdims=True) / jnp.sum(
        group_exp, axis=0, keepdims=True
    )
    expert_at = lax.broadcasted_iota(jnp.int32, expert_logits.shape, 0)
    logit_a = jnp.sum(jnp.where(expert_at == route_a, expert_logits, 0.0), axis=0, keepdims=True)
    logit_b = jnp.sum(jnp.where(expert_at == route_b, expert_logits, 0.0), axis=0, keepdims=True)
    top = jnp.maximum(logit_a, logit_b)
    exp_a, exp_b = jnp.exp(logit_a - top), jnp.exp(logit_b - top)
    gate_a = group_share * (exp_a / (exp_a + exp_b))
    gate_b = group_share * (exp_b / (exp_a + exp_b))
    base = jnp.sum(jnp.where(named, group_at * group_experts, 0), axis=0, keepdims=True)
    lane_at = lax.broadcasted_iota(jnp.int32, (LANES // 2, block), 0)
    share_t = jnp.where(lane_at == route_a - base, gate_a, 0.0) + jnp.where(
        lane_at == route_b - base, gate_b, 0.0
    )
    coarse = share_t.astype(jnp.bfloat16)
    fine = (share_t - coarse.astype(jnp.float32)).astype(jnp.bfloat16)
    row_at = lax.broadcasted_iota(jnp.int32, (block, block), 0)
    column_at = lax.broadcasted_iota(jnp.int32, (block, block), 1)
    earlier = jnp.where(row_at < column_at, 1.0, 0.0).astype(jnp.bfloat16)
    counts = jnp.dot(
        jnp.where(named, 1.0, 0.0).astype(jnp.bfloat16), earlier, preferred_element_type=jnp.float32
    )
    first_row = (group_at * chunk).astype(jnp.float32)
    place = jnp.sum(jnp.where(named, counts + first_row, 0.0), axis=0, keepdims=True)
    take = jnp.where(row_at.astype(jnp.float32) == place, 1.0, 0.0).astype(jnp.bfloat16)
    xs_ref[:, :depth] = jnp.dot(take, normed, preferred_element_type=jnp.float32).astype(
        jnp.bfloat16
    )
    xs_ref[:, depth:] = lax.dot_general(
        take, jnp.concatenate([coarse, fine], axis=0), across, preferred_element_type=jnp.float32
    ).astype(jnp.bfloat16)
    pl.semaphore_wait(barrier, len(peers))

    started = []

    def send(source, target, device):
        index = len(started)
        copy = pltpu.make_async_remote_copy(
            src_ref=source,
            dst_ref=target,
            send_sem=send_sem.at[index],
            recv_sem=recv_sem.at[index],
            device_id=device,
            device_id_type=MESH,
        )
        copy.start()
        started.append(copy)
        return copy

    my_chunk = pl.ds(pl.multiple_of(group * chunk, chunk), chunk)
    keep = pltpu.make_async_copy(xs_ref.at[my_chunk], rows.at[0, own], load_sem.at[4])
    keep.start()
    tail = pl.ds(row_count - WINDOW, WINDOW)
    halo = [
        send(source.at[:, tail], target.at[:, pl.ds(0, WINDOW)], next_dev)
        for source, target in ((k_ref, k_ext), (v_ref, v_ext))
    ]
    z_out = [keep]
    for step in range(1, groups):
        plane = (group + step) % groups
        there = pl.ds(pl.multiple_of(plane * chunk, chunk), chunk)
        z_out.append(send(xs_ref.at[there], rows.at[step, own], (plane * 2 + member, tp)))
    k_ext[:, pl.ds(WINDOW, row_count)] = k_ref[...]
    v_ext[:, pl.ds(WINDOW, row_count)] = v_ref[...]

    held = [dict() for _ in range(groups)]

    def stage_a(s):
        if s:
            z_out[s].wait_recv()
        else:
            keep.wait()
        held[s]["x"] = send(rows.at[s, own], rows.at[s, own], x_dev)
        held[s]["y"] = send(rows.at[s, own], rows.at[s, own], y_dev)

    def stage_b(s):
        held[s]["x"].wait_recv()
        held[s]["to_y"] = send(rows.at[s, slot_x], rows.at[s, slot_x], y_dev)

    def stage_c(s):
        held[s]["y"].wait_recv()
        held[s]["to_y"].wait_recv()
        held[s]["core"] = send(rows.at[s, mine_slots], rows.at[s, mine_slots], c_dev)

    def stage_d(s):
        held[s]["core"].wait_recv()
        batch = 8 * chunk
        tokens = rows[s, :, :, :depth].reshape(batch, depth)
        shares = rows[s, :, :, depth:].reshape(batch, LANES).astype(jnp.float32)
        lane = lax.broadcasted_iota(jnp.int32, shares.shape, 1) % (LANES // 2)

        def one(e, carry):
            share = jnp.sum(
                jnp.where(lane == member * wg.shape[0] + e, shares, 0.0), axis=1, keepdims=True
            )
            pre = jnp.dot(tokens, wg[e], preferred_element_type=jnp.float32)
            up = jnp.dot(tokens, wu[e], preferred_element_type=jnp.float32)
            act[e] = (jax.nn.silu(pre) * up * share).astype(jnp.bfloat16)
            return carry

        lax.fori_loop(0, wg.shape[0], one, 0)
        acts = jnp.concatenate([act[e] for e in range(wg.shape[0])], axis=1)
        tile = 512

        def column(n, carry):
            columns = pl.ds(pl.multiple_of(n * tile, tile), tile)
            value = jnp.dot(acts, wd[:, columns], preferred_element_type=jnp.float32)
            part[s, :, :, columns] = value.astype(jnp.bfloat16).reshape(8, chunk, tile)
            return carry

        lax.fori_loop(0, depth // tile, column, 0)
        held[s]["sum"] = send(part.at[s, other_slots], from_core.at[s], c_dev)

    def add(index, term):
        part[index] = (part[index].astype(jnp.float32) + term.astype(jnp.float32)).astype(
            jnp.bfloat16
        )

    def stage_e(s):
        held[s]["sum"].wait_recv()
        add((s, mine_slots), from_core[s])
        held[s]["d_y"] = send(part.at[s, slot_d, lo], relay_y.at[s], y_dev)
        held[s]["d_x"] = send(part.at[s, slot_d, hi], relay_x.at[s], x_dev)
        held[s]["x_hi"] = send(part.at[s, slot_x, hi], from_x.at[s, hi], x_dev)
        held[s]["y_lo"] = send(part.at[s, slot_y, lo], from_y.at[s, lo], y_dev)

    def stage_f(s):
        held[s]["d_y"].wait_recv()
        add((s, slot_x, lo), relay_y[s])
        held[s]["x_lo"] = send(part.at[s, slot_x, lo], from_x.at[s, lo], x_dev)
        held[s]["d_x"].wait_recv()
        add((s, slot_y, hi), relay_x[s])
        held[s]["y_hi"] = send(part.at[s, slot_y, hi], from_y.at[s, hi], y_dev)

    def stage_h(s):
        for name in ("x_hi", "y_lo", "x_lo", "y_hi"):
            held[s][name].wait_recv()
        summed = (
            part[s, own].astype(jnp.float32)
            + from_x[s].astype(jnp.float32)
            + from_y[s].astype(jnp.float32)
        ).astype(jnp.bfloat16)
        if s:
            total[s] = summed
            plane = (group + groups - s) % groups
            held[s]["home"] = send(total.at[s], back.at[my_chunk], (plane * 2 + member, tp))
        else:
            back[my_chunk] = summed

    head_count = q_ref.shape[1] // HD
    query_at = lax.broadcasted_iota(jnp.int32, (WINDOW, 2 * WINDOW), 0)
    key_at = lax.broadcasted_iota(jnp.int32, (WINDOW, 2 * WINDOW), 1)
    distance = query_at + WINDOW - key_at
    near = (distance >= 0) & (distance < WINDOW)

    def attend(b, carry):
        start = pl.multiple_of(b * WINDOW, WINDOW)
        keys = k_ext[:, pl.ds(start, 2 * WINDOW)]
        band = v_ext[:, pl.ds(start, 2 * WINDOW)]
        queries = q_ref[pl.ds(start, WINDOW)]
        allowed = near & (key_at + (ep * row_count + b * WINDOW - WINDOW) >= 0)
        outs = []
        for h in range(head_count):
            query = queries[:, h * HD : (h + 1) * HD]
            scores = jnp.dot(query, keys, preferred_element_type=jnp.float32) * HD ** (-0.5)
            masked = jnp.where(allowed, scores, -1e30)
            sink = jnp.full((WINDOW, 1), sink_ref[h], jnp.float32)
            row_max = jnp.maximum(jnp.max(masked, axis=1, keepdims=True), sink)
            weights = jnp.exp(masked - row_max)
            denominator = jnp.sum(weights, axis=1, keepdims=True) + jnp.exp(sink - row_max)
            probs = (weights * (1.0 / denominator)).astype(jnp.bfloat16)
            outs.append(lax.dot_general(probs, band, across, preferred_element_type=jnp.float32))
        heads[tp, pl.ds(start, WINDOW)] = jnp.concatenate(outs, axis=1).astype(jnp.bfloat16)
        return carry

    blocks = row_count // WINDOW
    piece = row_count // 4
    att_x = []

    def send_heads(i):
        span = pl.ds(i * piece, piece)
        att_x.append(send(heads.at[tp, span], heads.at[tp, span], x_dev))

    stage_a(0)
    lax.fori_loop(1, blocks // 2, attend, 0)
    stage_b(0)
    stage_a(1)
    lax.fori_loop(blocks // 2, blocks, attend, 0)
    stage_c(0)
    stage_b(1)
    stage_a(2)
    for copy in halo:
        copy.wait_recv()
    lax.fori_loop(0, 1, attend, 0)
    send_heads(0)
    att_c = send(heads.at[tp], heads.at[tp], c_dev)
    for load in loads:
        load.wait()
    stage_d(0)
    stage_c(1)
    stage_b(2)
    stage_a(3)
    stage_e(0)
    stage_d(1)
    send_heads(1)
    stage_f(0)
    stage_c(2)
    stage_b(3)
    stage_e(1)
    stage_d(2)
    stage_h(0)
    send_heads(2)
    stage_f(1)
    stage_c(3)
    stage_e(2)
    stage_d(3)
    stage_h(1)
    stage_f(2)
    stage_e(3)
    send_heads(3)
    stage_h(2)
    stage_f(3)
    for copy in att_x:
        copy.wait_recv()
    att_cx = send(heads.at[tp_x], heads.at[tp_x], c_dev)
    att_c.wait_recv()
    att_cx.wait_recv()
    stage_h(3)

    def project(i, carry):
        span = pl.ds(pl.multiple_of(i * piece, piece), piece)
        joined = jnp.concatenate([heads[t, span] for t in range(4)], axis=1)
        mixer_ref[span] = jnp.dot(joined, proj[...], preferred_element_type=jnp.float32).astype(
            jnp.bfloat16
        )
        return carry

    lax.fori_loop(0, 4, project, 0)
    for s in range(1, groups):
        held[s]["home"].wait_recv()
    out_ref[...] = lax.dot_general(
        take, back[...], (((0,), (0,)), ((), ())), preferred_element_type=jnp.float32
    ).astype(jnp.bfloat16)
    for copy in started:
        copy.wait_send()


def fused(
    sinks,
    q_heads,
    k_heads,
    v_heads,
    gain,
    router_group,
    router_expert,
    routes,
    tokens_b,
    expert_gate,
    expert_up,
    expert_down,
    proj,
):
    groups = router_group.shape[1]
    block = tokens_b.shape[0] // 4
    experts, depth, hidden = expert_gate.shape
    width = depth + LANES
    row_count, head_width = q_heads.shape
    down = expert_down.reshape(experts * hidden, depth)
    chunk = block // groups
    copies = 14 * groups + 8
    bf16 = jnp.bfloat16
    anywhere = pl.BlockSpec(memory_space=pl.ANY)
    vmem = pl.BlockSpec(memory_space=pltpu.VMEM)
    return pl.pallas_call(
        functools.partial(fused_kernel, groups),
        out_shape=(
            jax.ShapeDtypeStruct((row_count, proj.shape[1]), bf16),
            jax.ShapeDtypeStruct((block, depth), bf16),
        ),
        in_specs=[pl.BlockSpec(memory_space=pltpu.SMEM)] + [vmem] * 7 + [anywhere] * 5,
        out_specs=(vmem, vmem),
        scratch_shapes=[
            pltpu.VMEM((HD, row_count + WINDOW), bf16),
            pltpu.VMEM((HD, row_count + WINDOW), bf16),
            pltpu.VMEM((block, depth), bf16),
            pltpu.VMEM((block, width), bf16),
            pltpu.VMEM((4, row_count, head_width), bf16),
            pltpu.VMEM((groups, 8, chunk, width), bf16),
            pltpu.VMEM((groups, 8, chunk, depth), bf16),
            pltpu.VMEM(expert_gate.shape, bf16),
            pltpu.VMEM(expert_up.shape, bf16),
            pltpu.VMEM(down.shape, bf16),
            pltpu.VMEM(proj.shape, bf16),
            pltpu.VMEM((experts, 8 * chunk, hidden), bf16),
            pltpu.VMEM((groups, 4, chunk, depth), bf16),
            pltpu.VMEM((groups, chunk // 2, depth), bf16),
            pltpu.VMEM((groups, chunk // 2, depth), bf16),
            pltpu.VMEM((groups, chunk, depth), bf16),
            pltpu.VMEM((groups, chunk, depth), bf16),
            pltpu.VMEM((groups, chunk, depth), bf16),
            pltpu.VMEM((block, depth), bf16),
            pltpu.SemaphoreType.DMA((6,)),
            pltpu.SemaphoreType.DMA((copies,)),
            pltpu.SemaphoreType.DMA((copies,)),
        ],
        cost_estimate=pl.CostEstimate(
            flops=20_000_000_000, bytes_accessed=20_000_000, transcendentals=0
        ),
        compiler_params=pltpu.CompilerParams(
            collective_id=0, has_side_effects=True, vmem_limit_bytes=56 * 2**20
        ),
    )(
        sinks,
        q_heads,
        k_heads.T,
        v_heads.T,
        gain[None, :],
        router_group.T,
        router_expert.T,
        routes.T,
        tokens_b,
        expert_gate,
        expert_up,
        down,
        proj,
    )


def per_device(
    q_heads,
    k_heads,
    v_heads,
    sink_logits,
    out_weight,
    tokens_b,
    moe_gain,
    router_group,
    router_expert,
    route_expert,
    expert_gate,
    expert_up,
    expert_down,
):
    groups = router_group.shape[1]
    if (lax.axis_size("ep"), lax.axis_size("tp"), k_heads.shape[1]) == (2 * groups, 4, HD):
        return fused(
            sink_logits,
            q_heads,
            k_heads,
            v_heads,
            moe_gain,
            router_group,
            router_expert,
            route_expert,
            tokens_b,
            expert_gate,
            expert_up,
            expert_down,
            out_weight,
        )
    span_len = WINDOW
    row_count = q_heads.shape[0]
    kv_local = k_heads.shape[1] // HD
    group_size = HEADS // KV
    blocks = row_count // span_len
    stacked = jnp.stack([k_heads[row_count - span_len :], v_heads[row_count - span_len :]])
    earlier = shifted(stacked, "ep", 1)

    def make_band(own_rows, prev_rows):
        extended = jnp.concatenate([prev_rows, own_rows], axis=0).reshape(
            blocks + 1, span_len, kv_local, HD
        )
        return jnp.concatenate([extended[:-1], extended[1:]], axis=1)

    key_band = make_band(k_heads, earlier[0])
    value_band = make_band(v_heads, earlier[1])
    query_blocks = q_heads.reshape(blocks, span_len, kv_local, group_size, HD)
    scores = jnp.einsum(
        "nqhgd,nkhd->nhgqk", query_blocks, key_band, preferred_element_type=jnp.float32
    ) * HD ** (-0.5)
    first_row = lax.axis_index("ep") * row_count
    query_index = jnp.arange(span_len, dtype=jnp.int32)[:, None]
    key_index = jnp.arange(2 * span_len, dtype=jnp.int32)[None, :]
    distance = query_index + span_len - key_index
    key_place = (
        first_row
        + jnp.arange(blocks, dtype=jnp.int32)[:, None, None] * span_len
        + key_index[None]
        - span_len
    )
    allowed = (distance >= 0)[None] & (distance < span_len)[None] & (key_place >= 0)
    masked = jnp.where(allowed[:, None, None], scores, -1e30)
    sink_full = sink_logits.reshape(kv_local, group_size)[None, :, :, None]
    row_max = jnp.maximum(jnp.max(masked, axis=-1), sink_full)
    weights_exp = jnp.exp(masked - row_max[..., None])
    denominator = jnp.sum(weights_exp, axis=-1) + jnp.exp(sink_full - row_max)
    probs = (weights_exp / denominator[..., None]).astype(jnp.bfloat16)
    attended = jnp.einsum(
        "nhgqk,nkhd->nqhgd", probs, value_band, preferred_element_type=jnp.float32
    )
    attended = attended.astype(jnp.bfloat16).reshape(row_count, kv_local * group_size * HD)
    mixed = jnp.dot(
        lax.all_gather(attended, "tp", axis=1, tiled=True),
        out_weight,
        preferred_element_type=jnp.float32,
    )
    mixer_out = mixed.astype(jnp.bfloat16)
    tp_count = lax.axis_size("tp")
    tp_index = lax.axis_index("tp")
    exp_local = expert_gate.shape[0]
    expert_count = exp_local * lax.axis_size("ep")
    rows_dev = tokens_b.shape[0] // tp_count
    capacity = min(4 * rows_dev // expert_count, rows_dev // 4)
    own_routes = lax.dynamic_slice_in_dim(route_expert, tp_index * rows_dev, rows_dev, 0)
    own_normed = normalize(
        lax.dynamic_slice_in_dim(tokens_b, tp_index * rows_dev, rows_dev, 0), moe_gain
    )
    flat_routes, places = slot_positions(own_routes, 1, expert_count)
    buffer = fill_slots(own_normed, flat_routes, places, 1, expert_count, capacity, exp_local)
    delivered = lax.all_to_all(buffer, "ep", split_axis=0, concat_axis=0, tiled=True)
    arrived = lax.all_gather(delivered, "tp", axis=2, tiled=True)
    own_flat = flat_routes[0]
    own_places = places[0]
    gates = gate_weights(own_normed, own_routes, router_group, router_expert)
    gate_pre = jnp.einsum(
        "setcd,edf->setcf", arrived, expert_gate, preferred_element_type=jnp.float32
    )
    up_pre = jnp.einsum("setcd,edf->setcf", arrived, expert_up, preferred_element_type=jnp.float32)
    activated = (jax.nn.silu(gate_pre) * up_pre).astype(jnp.bfloat16)
    partial_value = jnp.einsum(
        "setcf,efd->setcd", activated, expert_down, preferred_element_type=jnp.float32
    )
    summed = lax.psum_scatter(
        partial_value.astype(jnp.bfloat16), "tp", scatter_dimension=2, tiled=True
    )
    returned = lax.all_to_all(summed, "ep", split_axis=0, concat_axis=0, tiled=True)
    returned = returned.reshape(expert_count * capacity, returned.shape[-1])
    picked_rows = returned[own_flat * capacity + own_places].reshape(
        rows_dev, 2, returned.shape[-1]
    )
    moe_out = jnp.sum(gates[:, :, None] * picked_rows.astype(jnp.float32), axis=1).astype(
        jnp.bfloat16
    )
    return (mixer_out, moe_out)


def solution(mesh):
    in_specs = (
        P("ep", "tp"),
        P("ep", "tp"),
        P("ep", "tp"),
        P("tp"),
        P(None, "tp"),
        P("ep", None),
        P(),
        P(),
        P(),
        P("ep", None),
        P("ep", None, "tp"),
        P("ep", None, "tp"),
        P("ep", "tp", None),
    )
    out_specs = (P("ep", "tp"), P(("ep", "tp"), None))
    return jax.shard_map(
        per_device, mesh=mesh, in_specs=in_specs, out_specs=out_specs, check_vma=False
    )
```

```python
import functools

import jax
import jax.numpy as jnp
from jax import lax
from jax.experimental import pallas as pl
from jax.experimental.pallas import tpu as pltpu
from jax.sharding import PartitionSpec as P

HEADS = 16
KV = 4
HD = 64
WINDOW = 128


def shifted(value, axis, steps):
    count = lax.axis_size(axis)
    leading, last = (max(0, -steps), min(count, count - steps))
    return lax.ppermute(value, axis, [(source, source + steps) for source in range(leading, last)])


def normalize(rows_in, gain):
    values = rows_in.astype(jnp.float32)
    scaled = values * lax.rsqrt(jnp.mean(values * values, axis=-1, keepdims=True) + 1e-06) * gain
    return scaled.astype(jnp.bfloat16)


def gate_weights(normed, routes, router_group, router_expert):
    group_logits = jnp.dot(normed, router_group, preferred_element_type=jnp.float32)
    expert_logits = jnp.dot(normed, router_expert, preferred_element_type=jnp.float32)
    group_count = router_group.shape[1]
    expert_count = router_expert.shape[1]
    chosen_group = routes[:, 0] // (expert_count // group_count)
    group_match = chosen_group[:, None] == jnp.arange(group_count, dtype=jnp.int32)[None, :]
    group_share = jnp.sum(
        jnp.where(group_match, jax.nn.softmax(group_logits, axis=-1), 0.0), axis=-1
    )
    expert_match = routes[:, :, None] == jnp.arange(expert_count, dtype=jnp.int32)[None, None, :]
    picked = jnp.sum(jnp.where(expert_match, expert_logits[:, None, :], 0.0), axis=-1)
    return group_share[:, None] * jax.nn.softmax(picked, axis=-1)


def slot_positions(routes, sub_count, expert_count):
    flat_routes = routes.reshape(sub_count, -1)
    onehot = (
        flat_routes[:, :, None] == jnp.arange(expert_count, dtype=jnp.int32)[None, None, :]
    ).astype(jnp.int32)
    places = jnp.sum(onehot * jnp.cumsum(onehot, axis=1), axis=2) - 1
    return (flat_routes, places)


def fill_slots(normed, flat_routes, places, sub_count, expert_count, capacity, exp_local):
    sub_index = jnp.arange(sub_count, dtype=jnp.int32)[:, None]
    target = ((flat_routes * sub_count + sub_index) * capacity + places).reshape(-1)
    source = jnp.repeat(normed, 2, axis=0)
    buffer = jnp.zeros((expert_count * sub_count * capacity, normed.shape[1]), jnp.bfloat16)
    buffer = buffer.at[target].set(source)
    return buffer.reshape(
        expert_count // exp_local, exp_local, sub_count, capacity, normed.shape[1]
    )


LANES = 128
MESH = pl.DeviceIdType.MESH


def fused_kernel(
    groups,
    sink_ref,
    q_ref,
    k_ref,
    v_ref,
    gain_ref,
    group_ref,
    expert_ref,
    route_ref,
    tokens_hbm,
    gate_hbm,
    up_hbm,
    down_hbm,
    proj_hbm,
    mixer_ref,
    out_ref,
    k_ext,
    v_ext,
    tokens,
    xs_ref,
    heads,
    rows,
    part,
    wg,
    wu,
    wd,
    proj,
    act,
    from_core,
    relay_x,
    relay_y,
    from_x,
    from_y,
    total,
    back,
    load_sem,
    send_sem,
    recv_sem,
):
    ep, tp = lax.axis_index("ep"), lax.axis_index("tp")
    group, member = ep // 2, ep % 2
    x, core = tp // 2, tp % 2
    tp_x, tp_c = (1 - x) * 2 + core, x * 2 + (1 - core)
    ep_y = group * 2 + (1 - member)
    ep_count = groups * 2
    x_dev, y_dev, c_dev = (ep, tp_x), (ep_y, tp), (ep, tp_c)
    next_dev = ((ep + 1) % ep_count, tp)
    prev_dev = ((ep + ep_count - 1) % ep_count, tp)
    depth = out_ref.shape[1]
    chunk = xs_ref.shape[0] // groups
    half = chunk // 2
    row_count = q_ref.shape[0]
    lo, hi = pl.ds(0, half), pl.ds(half, half)
    mine, other = core * 4, (1 - core) * 4
    own = mine + member * 2 + x
    slot_x = mine + member * 2 + (1 - x)
    slot_y = mine + (1 - member) * 2 + x
    slot_d = mine + (1 - member) * 2 + (1 - x)
    mine_slots, other_slots = pl.ds(mine, 4), pl.ds(other, 4)

    pairs = ((gate_hbm, wg), (up_hbm, wu), (down_hbm, wd), (proj_hbm, proj))
    loads = [
        pltpu.make_async_copy(source, held, load_sem.at[i])
        for i, (source, held) in enumerate(pairs)
    ]
    block = xs_ref.shape[0]
    first = pl.multiple_of(tp * block, block)
    fetch = pltpu.make_async_copy(tokens_hbm.at[pl.ds(first, block)], tokens, load_sem.at[5])
    fetch.start()
    for load in loads:
        load.start()

    barrier = pltpu.get_barrier_semaphore()
    ahead = [((group + step) % groups) * 2 + member for step in range(1, groups)]
    peers = [(plane, tp) for plane in ahead] + [x_dev, y_dev, c_dev, next_dev, prev_dev]
    for peer in peers:
        pl.semaphore_signal(barrier, inc=1, device_id=peer, device_id_type=MESH)
    fetch.wait()
    values = tokens[...].astype(jnp.float32)
    scale = lax.rsqrt(jnp.mean(values * values, axis=1, keepdims=True) + 1e-06)
    normed = (values * scale * gain_ref[...]).astype(jnp.bfloat16)
    across = (((1,), (1,)), ((), ()))
    group_logits = lax.dot_general(
        group_ref[...], normed, across, preferred_element_type=jnp.float32
    )
    expert_logits = lax.dot_general(
        expert_ref[...], normed, across, preferred_element_type=jnp.float32
    )
    routes = route_ref[:, pl.ds(first, block)]
    route_a, route_b = routes[0:1], routes[1:2]
    group_experts = expert_ref.shape[0] // groups
    group_at = lax.broadcasted_iota(jnp.int32, (groups, block), 0)
    inside = route_a - group_at * group_experts
    named = (inside >= 0) & (inside < group_experts)
    group_exp = jnp.exp(group_logits - jnp.max(group_logits, axis=0, keepdims=True))
    group_share = jnp.sum(jnp.where(named, group_exp, 0.0), axis=0, keepdims=True) / jnp.sum(
        group_exp, axis=0, keepdims=True
    )
    expert_at = lax.broadcasted_iota(jnp.int32, expert_logits.shape, 0)
    logit_a = jnp.sum(jnp.where(expert_at == route_a, expert_logits, 0.0), axis=0, keepdims=True)
    logit_b = jnp.sum(jnp.where(expert_at == route_b, expert_logits, 0.0), axis=0, keepdims=True)
    top = jnp.maximum(logit_a, logit_b)
    exp_a, exp_b = jnp.exp(logit_a - top), jnp.exp(logit_b - top)
    gate_a = group_share * (exp_a / (exp_a + exp_b))
    gate_b = group_share * (exp_b / (exp_a + exp_b))
    base = jnp.sum(jnp.where(named, group_at * group_experts, 0), axis=0, keepdims=True)
    lane_at = lax.broadcasted_iota(jnp.int32, (LANES // 2, block), 0)
    share_t = jnp.where(lane_at == route_a - base, gate_a, 0.0) + jnp.where(
        lane_at == route_b - base, gate_b, 0.0
    )
    coarse = share_t.astype(jnp.bfloat16)
    fine = (share_t - coarse.astype(jnp.float32)).astype(jnp.bfloat16)
    row_at = lax.broadcasted_iota(jnp.int32, (block, block), 0)
    column_at = lax.broadcasted_iota(jnp.int32, (block, block), 1)
    earlier = jnp.where(row_at < column_at, 1.0, 0.0).astype(jnp.bfloat16)
    counts = jnp.dot(
        jnp.where(named, 1.0, 0.0).astype(jnp.bfloat16), earlier, preferred_element_type=jnp.float32
    )
    first_row = (group_at * chunk).astype(jnp.float32)
    place = jnp.sum(jnp.where(named, counts + first_row, 0.0), axis=0, keepdims=True)
    take = jnp.where(row_at.astype(jnp.float32) == place, 1.0, 0.0).astype(jnp.bfloat16)
    xs_ref[:, :depth] = jnp.dot(take, normed, preferred_element_type=jnp.float32).astype(
        jnp.bfloat16
    )
    xs_ref[:, depth:] = lax.dot_general(
        take, jnp.concatenate([coarse, fine], axis=0), across, preferred_element_type=jnp.float32
    ).astype(jnp.bfloat16)
    pl.semaphore_wait(barrier, len(peers))

    started = []

    def send(source, target, device):
        index = len(started)
        copy = pltpu.make_async_remote_copy(
            src_ref=source,
            dst_ref=target,
            send_sem=send_sem.at[index],
            recv_sem=recv_sem.at[index],
            device_id=device,
            device_id_type=MESH,
        )
        copy.start()
        started.append(copy)
        return copy

    my_chunk = pl.ds(pl.multiple_of(group * chunk, chunk), chunk)
    keep = pltpu.make_async_copy(xs_ref.at[my_chunk], rows.at[0, own], load_sem.at[4])
    keep.start()
    tail = pl.ds(row_count - WINDOW, WINDOW)
    halo = [
        send(source.at[:, tail], target.at[:, pl.ds(0, WINDOW)], next_dev)
        for source, target in ((k_ref, k_ext), (v_ref, v_ext))
    ]
    z_out = [keep]
    for step in range(1, groups):
        plane = (group + step) % groups
        there = pl.ds(pl.multiple_of(plane * chunk, chunk), chunk)
        z_out.append(send(xs_ref.at[there], rows.at[step, own], (plane * 2 + member, tp)))
    k_ext[:, pl.ds(WINDOW, row_count)] = k_ref[...]
    v_ext[:, pl.ds(WINDOW, row_count)] = v_ref[...]

    held = [dict() for _ in range(groups)]

    def stage_a(s):
        if s:
            z_out[s].wait_recv()
        else:
            keep.wait()
        held[s]["x"] = send(rows.at[s, own], rows.at[s, own], x_dev)
        held[s]["y"] = send(rows.at[s, own], rows.at[s, own], y_dev)

    def stage_b(s):
        held[s]["x"].wait_recv()
        held[s]["to_y"] = send(rows.at[s, slot_x], rows.at[s, slot_x], y_dev)

    def stage_c(s):
        held[s]["y"].wait_recv()
        held[s]["to_y"].wait_recv()
        held[s]["core"] = send(rows.at[s, mine_slots], rows.at[s, mine_slots], c_dev)

    def stage_d(s):
        held[s]["core"].wait_recv()
        batch = 8 * chunk
        tokens = rows[s, :, :, :depth].reshape(batch, depth)
        shares = rows[s, :, :, depth:].reshape(batch, LANES).astype(jnp.float32)
        lane = lax.broadcasted_iota(jnp.int32, shares.shape, 1) % (LANES // 2)

        def one(e, carry):
            share = jnp.sum(
                jnp.where(lane == member * wg.shape[0] + e, shares, 0.0), axis=1, keepdims=True
            )
            pre = jnp.dot(tokens, wg[e], preferred_element_type=jnp.float32)
            up = jnp.dot(tokens, wu[e], preferred_element_type=jnp.float32)
            act[e] = (jax.nn.silu(pre) * up * share).astype(jnp.bfloat16)
            return carry

        lax.fori_loop(0, wg.shape[0], one, 0)
        acts = jnp.concatenate([act[e] for e in range(wg.shape[0])], axis=1)
        tile = 512

        def column(n, carry):
            columns = pl.ds(pl.multiple_of(n * tile, tile), tile)
            value = jnp.dot(acts, wd[:, columns], preferred_element_type=jnp.float32)
            part[s, :, :, columns] = value.astype(jnp.bfloat16).reshape(8, chunk, tile)
            return carry

        lax.fori_loop(0, depth // tile, column, 0)
        held[s]["sum"] = send(part.at[s, other_slots], from_core.at[s], c_dev)

    def add(index, term):
        part[index] = (part[index].astype(jnp.float32) + term.astype(jnp.float32)).astype(
            jnp.bfloat16
        )

    def stage_e(s):
        held[s]["sum"].wait_recv()
        add((s, mine_slots), from_core[s])
        held[s]["d_y"] = send(part.at[s, slot_d, lo], relay_y.at[s], y_dev)
        held[s]["d_x"] = send(part.at[s, slot_d, hi], relay_x.at[s], x_dev)
        held[s]["x_hi"] = send(part.at[s, slot_x, hi], from_x.at[s, hi], x_dev)
        held[s]["y_lo"] = send(part.at[s, slot_y, lo], from_y.at[s, lo], y_dev)

    def stage_f(s):
        held[s]["d_y"].wait_recv()
        add((s, slot_x, lo), relay_y[s])
        held[s]["x_lo"] = send(part.at[s, slot_x, lo], from_x.at[s, lo], x_dev)
        held[s]["d_x"].wait_recv()
        add((s, slot_y, hi), relay_x[s])
        held[s]["y_hi"] = send(part.at[s, slot_y, hi], from_y.at[s, hi], y_dev)

    def stage_h(s):
        for name in ("x_hi", "y_lo", "x_lo", "y_hi"):
            held[s][name].wait_recv()
        summed = (
            part[s, own].astype(jnp.float32)
            + from_x[s].astype(jnp.float32)
            + from_y[s].astype(jnp.float32)
        ).astype(jnp.bfloat16)
        if s:
            total[s] = summed
            plane = (group + groups - s) % groups
            held[s]["home"] = send(total.at[s], back.at[my_chunk], (plane * 2 + member, tp))
        else:
            back[my_chunk] = summed

    head_count = q_ref.shape[1] // HD
    query_at = lax.broadcasted_iota(jnp.int32, (WINDOW, 2 * WINDOW), 0)
    key_at = lax.broadcasted_iota(jnp.int32, (WINDOW, 2 * WINDOW), 1)
    distance = query_at + WINDOW - key_at
    near = (distance >= 0) & (distance < WINDOW)

    def attend(b, carry):
        start = pl.multiple_of(b * WINDOW, WINDOW)
        keys = k_ext[:, pl.ds(start, 2 * WINDOW)]
        band = v_ext[:, pl.ds(start, 2 * WINDOW)]
        queries = q_ref[pl.ds(start, WINDOW)]
        allowed = near & (key_at + (ep * row_count + b * WINDOW - WINDOW) >= 0)
        outs = []
        for h in range(head_count):
            query = queries[:, h * HD : (h + 1) * HD]
            scores = jnp.dot(query, keys, preferred_element_type=jnp.float32) * HD ** (-0.5)
            masked = jnp.where(allowed, scores, -1e30)
            sink = jnp.full((WINDOW, 1), sink_ref[h], jnp.float32)
            row_max = jnp.maximum(jnp.max(masked, axis=1, keepdims=True), sink)
            weights = jnp.exp(masked - row_max)
            denominator = jnp.sum(weights, axis=1, keepdims=True) + jnp.exp(sink - row_max)
            probs = (weights * (1.0 / denominator)).astype(jnp.bfloat16)
            outs.append(lax.dot_general(probs, band, across, preferred_element_type=jnp.float32))
        heads[tp, pl.ds(start, WINDOW)] = jnp.concatenate(outs, axis=1).astype(jnp.bfloat16)
        return carry

    blocks = row_count // WINDOW
    piece = row_count // 4
    att_x = []

    def send_heads(i):
        span = pl.ds(i * piece, piece)
        att_x.append(send(heads.at[tp, span], heads.at[tp, span], x_dev))

    stage_a(0)
    lax.fori_loop(1, blocks // 2, attend, 0)
    stage_b(0)
    stage_a(1)
    lax.fori_loop(blocks // 2, blocks, attend, 0)
    stage_c(0)
    stage_b(1)
    stage_a(2)
    def project(i, carry):
        span = pl.ds(pl.multiple_of(i * piece, piece), piece)
        joined = jnp.concatenate([heads[t, span] for t in range(4)], axis=1)
        mixer_ref[span] = jnp.dot(joined, proj[...], preferred_element_type=jnp.float32).astype(
            jnp.bfloat16
        )
        return carry

    for copy in halo:
        copy.wait_recv()
    lax.fori_loop(0, 1, attend, 0)
    att_c = send(heads.at[tp], heads.at[tp], c_dev)
    stage_a(3)
    send_heads(0)
    send_heads(1)
    for load in loads:
        load.wait()
    stage_d(0)
    stage_c(1)
    stage_b(2)
    send_heads(2)
    send_heads(3)
    stage_e(0)
    stage_d(1)
    stage_c(2)
    stage_b(3)
    stage_e(1)
    stage_f(0)
    stage_d(2)
    stage_c(3)
    stage_e(2)
    stage_f(1)
    stage_h(0)
    stage_d(3)
    stage_e(3)
    for copy in att_x:
        copy.wait_recv()
    att_cx = send(heads.at[tp_x], heads.at[tp_x], c_dev)
    stage_f(2)
    stage_h(1)
    stage_f(3)
    stage_h(2)
    att_c.wait_recv()
    att_cx.wait_recv()
    lax.fori_loop(0, 4, project, 0)
    stage_h(3)
    for s in range(1, groups):
        held[s]["home"].wait_recv()
    out_ref[...] = lax.dot_general(
        take, back[...], (((0,), (0,)), ((), ())), preferred_element_type=jnp.float32
    ).astype(jnp.bfloat16)
    for copy in started:
        copy.wait_send()


def fused(
    sinks,
    q_heads,
    k_heads,
    v_heads,
    gain,
    router_group,
    router_expert,
    routes,
    tokens_b,
    expert_gate,
    expert_up,
    expert_down,
    proj,
):
    groups = router_group.shape[1]
    block = tokens_b.shape[0] // 4
    experts, depth, hidden = expert_gate.shape
    width = depth + LANES
    row_count, head_width = q_heads.shape
    down = expert_down.reshape(experts * hidden, depth)
    chunk = block // groups
    copies = 14 * groups + 8
    bf16 = jnp.bfloat16
    anywhere = pl.BlockSpec(memory_space=pl.ANY)
    vmem = pl.BlockSpec(memory_space=pltpu.VMEM)
    return pl.pallas_call(
        functools.partial(fused_kernel, groups),
        out_shape=(
            jax.ShapeDtypeStruct((row_count, proj.shape[1]), bf16),
            jax.ShapeDtypeStruct((block, depth), bf16),
        ),
        in_specs=[pl.BlockSpec(memory_space=pltpu.SMEM)] + [vmem] * 7 + [anywhere] * 5,
        out_specs=(vmem, vmem),
        scratch_shapes=[
            pltpu.VMEM((HD, row_count + WINDOW), bf16),
            pltpu.VMEM((HD, row_count + WINDOW), bf16),
            pltpu.VMEM((block, depth), bf16),
            pltpu.VMEM((block, width), bf16),
            pltpu.VMEM((4, row_count, head_width), bf16),
            pltpu.VMEM((groups, 8, chunk, width), bf16),
            pltpu.VMEM((groups, 8, chunk, depth), bf16),
            pltpu.VMEM(expert_gate.shape, bf16),
            pltpu.VMEM(expert_up.shape, bf16),
            pltpu.VMEM(down.shape, bf16),
            pltpu.VMEM(proj.shape, bf16),
            pltpu.VMEM((experts, 8 * chunk, hidden), bf16),
            pltpu.VMEM((groups, 4, chunk, depth), bf16),
            pltpu.VMEM((groups, chunk // 2, depth), bf16),
            pltpu.VMEM((groups, chunk // 2, depth), bf16),
            pltpu.VMEM((groups, chunk, depth), bf16),
            pltpu.VMEM((groups, chunk, depth), bf16),
            pltpu.VMEM((groups, chunk, depth), bf16),
            pltpu.VMEM((block, depth), bf16),
            pltpu.SemaphoreType.DMA((6,)),
            pltpu.SemaphoreType.DMA((copies,)),
            pltpu.SemaphoreType.DMA((copies,)),
        ],
        cost_estimate=pl.CostEstimate(
            flops=20_000_000_000, bytes_accessed=20_000_000, transcendentals=0
        ),
        compiler_params=pltpu.CompilerParams(
            collective_id=0, has_side_effects=True, vmem_limit_bytes=56 * 2**20
        ),
    )(
        sinks,
        q_heads,
        k_heads.T,
        v_heads.T,
        gain[None, :],
        router_group.T,
        router_expert.T,
        routes.T,
        tokens_b,
        expert_gate,
        expert_up,
        down,
        proj,
    )


def per_device(
    q_heads,
    k_heads,
    v_heads,
    sink_logits,
    out_weight,
    tokens_b,
    moe_gain,
    router_group,
    router_expert,
    route_expert,
    expert_gate,
    expert_up,
    expert_down,
):
    groups = router_group.shape[1]
    if (lax.axis_size("ep"), lax.axis_size("tp"), k_heads.shape[1]) == (2 * groups, 4, HD):
        return fused(
            sink_logits,
            q_heads,
            k_heads,
            v_heads,
            moe_gain,
            router_group,
            router_expert,
            route_expert,
            tokens_b,
            expert_gate,
            expert_up,
            expert_down,
            out_weight,
        )
    span_len = WINDOW
    row_count = q_heads.shape[0]
    kv_local = k_heads.shape[1] // HD
    group_size = HEADS // KV
    blocks = row_count // span_len
    stacked = jnp.stack([k_heads[row_count - span_len :], v_heads[row_count - span_len :]])
    earlier = shifted(stacked, "ep", 1)

    def make_band(own_rows, prev_rows):
        extended = jnp.concatenate([prev_rows, own_rows], axis=0).reshape(
            blocks + 1, span_len, kv_local, HD
        )
        return jnp.concatenate([extended[:-1], extended[1:]], axis=1)

    key_band = make_band(k_heads, earlier[0])
    value_band = make_band(v_heads, earlier[1])
    query_blocks = q_heads.reshape(blocks, span_len, kv_local, group_size, HD)
    scores = jnp.einsum(
        "nqhgd,nkhd->nhgqk", query_blocks, key_band, preferred_element_type=jnp.float32
    ) * HD ** (-0.5)
    first_row = lax.axis_index("ep") * row_count
    query_index = jnp.arange(span_len, dtype=jnp.int32)[:, None]
    key_index = jnp.arange(2 * span_len, dtype=jnp.int32)[None, :]
    distance = query_index + span_len - key_index
    key_place = (
        first_row
        + jnp.arange(blocks, dtype=jnp.int32)[:, None, None] * span_len
        + key_index[None]
        - span_len
    )
    allowed = (distance >= 0)[None] & (distance < span_len)[None] & (key_place >= 0)
    masked = jnp.where(allowed[:, None, None], scores, -1e30)
    sink_full = sink_logits.reshape(kv_local, group_size)[None, :, :, None]
    row_max = jnp.maximum(jnp.max(masked, axis=-1), sink_full)
    weights_exp = jnp.exp(masked - row_max[..., None])
    denominator = jnp.sum(weights_exp, axis=-1) + jnp.exp(sink_full - row_max)
    probs = (weights_exp / denominator[..., None]).astype(jnp.bfloat16)
    attended = jnp.einsum(
        "nhgqk,nkhd->nqhgd", probs, value_band, preferred_element_type=jnp.float32
    )
    attended = attended.astype(jnp.bfloat16).reshape(row_count, kv_local * group_size * HD)
    mixed = jnp.dot(
        lax.all_gather(attended, "tp", axis=1, tiled=True),
        out_weight,
        preferred_element_type=jnp.float32,
    )
    mixer_out = mixed.astype(jnp.bfloat16)
    tp_count = lax.axis_size("tp")
    tp_index = lax.axis_index("tp")
    exp_local = expert_gate.shape[0]
    expert_count = exp_local * lax.axis_size("ep")
    rows_dev = tokens_b.shape[0] // tp_count
    capacity = min(4 * rows_dev // expert_count, rows_dev // 4)
    own_routes = lax.dynamic_slice_in_dim(route_expert, tp_index * rows_dev, rows_dev, 0)
    own_normed = normalize(
        lax.dynamic_slice_in_dim(tokens_b, tp_index * rows_dev, rows_dev, 0), moe_gain
    )
    flat_routes, places = slot_positions(own_routes, 1, expert_count)
    buffer = fill_slots(own_normed, flat_routes, places, 1, expert_count, capacity, exp_local)
    delivered = lax.all_to_all(buffer, "ep", split_axis=0, concat_axis=0, tiled=True)
    arrived = lax.all_gather(delivered, "tp", axis=2, tiled=True)
    own_flat = flat_routes[0]
    own_places = places[0]
    gates = gate_weights(own_normed, own_routes, router_group, router_expert)
    gate_pre = jnp.einsum(
        "setcd,edf->setcf", arrived, expert_gate, preferred_element_type=jnp.float32
    )
    up_pre = jnp.einsum("setcd,edf->setcf", arrived, expert_up, preferred_element_type=jnp.float32)
    activated = (jax.nn.silu(gate_pre) * up_pre).astype(jnp.bfloat16)
    partial_value = jnp.einsum(
        "setcf,efd->setcd", activated, expert_down, preferred_element_type=jnp.float32
    )
    summed = lax.psum_scatter(
        partial_value.astype(jnp.bfloat16), "tp", scatter_dimension=2, tiled=True
    )
    returned = lax.all_to_all(summed, "ep", split_axis=0, concat_axis=0, tiled=True)
    returned = returned.reshape(expert_count * capacity, returned.shape[-1])
    picked_rows = returned[own_flat * capacity + own_places].reshape(
        rows_dev, 2, returned.shape[-1]
    )
    moe_out = jnp.sum(gates[:, :, None] * picked_rows.astype(jnp.float32), axis=1).astype(
        jnp.bfloat16
    )
    return (mixer_out, moe_out)


def solution(mesh):
    in_specs = (
        P("ep", "tp"),
        P("ep", "tp"),
        P("ep", "tp"),
        P("tp"),
        P(None, "tp"),
        P("ep", None),
        P(),
        P(),
        P(),
        P("ep", None),
        P("ep", None, "tp"),
        P("ep", None, "tp"),
        P("ep", "tp", None),
    )
    out_specs = (P("ep", "tp"), P(("ep", "tp"), None))
    return jax.shard_map(
        per_device, mesh=mesh, in_specs=in_specs, out_specs=out_specs, check_vma=False
    )
```
